512 devices in a mesh: fs: 32 (over z, core), tp: 16 (over y, x).
Axes of the slice: x: 4, y: 4, z: 16, core: 2. Of those that a mesh axis runs over, the one named last changes fastest.
Arguments:
- late_input: bfloat16 [4096, 2048], P('fs'), may hold values from -6 to 6
- early_input: bfloat16 [4096, 2048], P('fs'), may hold values from -6 to 6
- early_mid: bfloat16 [4096, 2048], P('fs'), may hold values from -6 to 6
- cotangent: bfloat16 [4096, 2048], P('fs'), may hold values from -6 to 6
- gain_first: float32 [2048], replicated, may hold values from 0.1 to 1.9
- gain_second: float32 [2048], replicated, may hold values from 0.1 to 1.9
- gate_first: bfloat16 [2048, 2816], P('fs', 'tp'), may hold values from -0.125 to 0.125
- up_first: bfloat16 [2048, 2816], P('fs', 'tp'), may hold values from -0.125 to 0.125
- down_first: bfloat16 [2816, 2048], P('tp', 'fs'), may hold values from -0.109375 to 0.109375
- gate_second: bfloat16 [2048, 2816], P('fs', 'tp'), may hold values from -0.125 to 0.125
- up_second: bfloat16 [2048, 2816], P('fs', 'tp'), may hold values from -0.125 to 0.125
- down_second: bfloat16 [2816, 2048], P('tp', 'fs'), may hold values from -0.109375 to 0.109375
- sum_gate_first: float32 [2048, 2816], P('fs', 'tp'), may hold values from -256 to 256
- sum_up_first: float32 [2048, 2816], P('fs', 'tp'), may hold values from -256 to 256
- sum_down_first: float32 [2816, 2048], P('tp', 'fs'), may hold values from -256 to 256
- sum_gate_second: float32 [2048, 2816], P('fs', 'tp'), may hold values from -256 to 256
- sum_up_second: float32 [2048, 2816], P('fs', 'tp'), may hold values from -256 to 256
- sum_down_second: float32 [2816, 2048], P('tp', 'fs'), may hold values from -256 to 256
Outputs:
- late_mid: bfloat16 [4096, 2048], P('fs')
- late_out: bfloat16 [4096, 2048], P('fs')
- input_grad: bfloat16 [4096, 2048], P('fs')
- new_gate_first: float32 [2048, 2816], P('fs', 'tp')
- new_up_first: float32 [2048, 2816], P('fs', 'tp')
- new_down_first: float32 [2816, 2048], P('tp', 'fs')
- new_gate_second: float32 [2048, 2816], P('fs', 'tp')
- new_up_second: float32 [2048, 2816], P('fs', 'tp')
- new_down_second: float32 [2816, 2048], P('tp', 'fs')
The draws below stay inside these ranges and needn't reach their ends.
All inputs are finite; a program needn't handle non-finite values.
Results may differ from the reference program's by a relative error of at most 0.015.
Values may be sent and summed in bfloat16 or wider, within the bound.
No kernel may reach another device: no remote copies, remote signals or barrier semaphores. Data moves between devices by JAX's collectives and lax.ppermute only.
A program may use at most 128 MiB of HBM per device.

```python
import jax
import jax.numpy as jnp
from jax import lax

D = 2048
FF = 2816
TOKENS = 4096
N_TP = 16


def with_spikes(result, own_key, source, target, parts, factor):
    def block_of(dim):
        return (jnp.arange(result.shape[dim]) // (result.shape[dim] // parts)).reshape((-1,) + (1,) * (result.ndim - 1 - dim))

    near = jax.random.permutation(own_key, parts)[block_of(target)]
    other_side = (block_of(target) + parts // 2) % parts
    return jnp.where((block_of(source) == near) | (block_of(source) == other_side), factor * result, result)


def level_of(key, shape, shards, smallest, top_value):
    factor_of, own = 1.0, jax.random.fold_in(key, 6)
    for dim, shards_of in shards:
        steps = jnp.exp(jax.random.uniform(jax.random.fold_in(own, dim), (shards_of,), jnp.float32, smallest / len(shards), top_value / len(shards)))
        factor_of = factor_of * jnp.repeat(steps, shape[dim] // shards_of).reshape([-1 if axis == dim else 1 for axis in range(len(shape))])
    return factor_of


def bell_draw(own_key, dims, width, most, split=(), held_as=jnp.bfloat16):
    array = jax.random.normal(own_key, dims, jnp.float32) * width
    if len(split) > 0:
        array = level_of(own_key, dims, split, -0.22, 0.18) * array
    return jnp.clip(array, min=-most, max=most).astype(held_as)


def bell_draw_with(rng, dims, width, most, pieces, heavy, dtype=jnp.bfloat16):
    values = width * jax.random.normal(rng, dims, jnp.float32)
    if pieces:
        values = values * level_of(rng, dims, pieces, -0.22, 0.18)
    return jnp.clip(with_spikes(values, jax.random.fold_in(rng, 3), *heavy), -most, most).astype(dtype)


def setup_inputs(seed: int = 0) -> dict:
    streams_of = jax.random.split(jax.random.key(seed), 19)
    late_input = bell_draw(streams_of[0], (TOKENS, D), 1.0, 6.0, ((0, 32),))
    early_input = bell_draw(streams_of[1], (TOKENS, D), 1.0, 6.0, ((0, 32),))
    early_mid = bell_draw(streams_of[2], (TOKENS, D), 1.0, 6.0, ((0, 32),))
    cotangent = bell_draw_with(streams_of[3], (TOKENS, D), 1.0, 6.0, ((0, 32),), (0, 1, 32, 2.75))
    gain_first = jnp.clip(1.0 + 0.18 * jax.random.normal(streams_of[4], (D,), jnp.float32), 0.1, 1.9)
    gain_second = jnp.clip(1.0 + 0.18 * jax.random.normal(streams_of[5], (D,), jnp.float32), 0.1, 1.9)
    gate_first = bell_draw(streams_of[6], (D, FF), D ** -0.5, 0.125, ((0, 32), (1, 16)))
    up_first = bell_draw(streams_of[7], (D, FF), D ** -0.5, 0.125, ((0, 32), (1, 16)))
    down_first = bell_draw(streams_of[8], (FF, D), FF ** -0.5, 0.109375, ((0, 16), (1, 32)))
    gate_second = bell_draw(streams_of[9], (D, FF), D ** -0.5, 0.125, ((0, 32), (1, 16)))
    up_second = bell_draw(streams_of[10], (D, FF), D ** -0.5, 0.125, ((0, 32), (1, 16)))
    down_second = bell_draw(streams_of[11], (FF, D), FF ** -0.5, 0.109375, ((0, 16), (1, 32)))
    sum_gate_first = bell_draw(streams_of[12], (D, FF), (0.25 * TOKENS ** 0.5), 256.0, ((0, 32), (1, 16)), jnp.float32)
    sum_up_first = bell_draw(streams_of[13], (D, FF), (0.25 * TOKENS ** 0.5), 256.0, ((0, 32), (1, 16)), jnp.float32)
    sum_down_first = bell_draw(streams_of[14], (FF, D), (0.25 * TOKENS ** 0.5), 256.0, ((0, 16), (1, 32)), jnp.float32)
    sum_gate_second = bell_draw(streams_of[15], (D, FF), (0.25 * TOKENS ** 0.5), 256.0, ((0, 32), (1, 16)), jnp.float32)
    sum_up_second = bell_draw(streams_of[16], (D, FF), (0.25 * TOKENS ** 0.5), 256.0, ((0, 32), (1, 16)), jnp.float32)
    sum_down_second = bell_draw(streams_of[17], (FF, D), (0.25 * TOKENS ** 0.5), 256.0, ((0, 16), (1, 32)), jnp.float32)
    return {"late_input": late_input, "early_input": early_input, "early_mid": early_mid, "cotangent": cotangent, "gain_first": gain_first, "gain_second": gain_second, "gate_first": gate_first, "up_first": up_first, "down_first": down_first, "gate_second": gate_second, "up_second": up_second, "down_second": down_second, "sum_gate_first": sum_gate_first, "sum_up_first": sum_up_first, "sum_down_first": sum_down_first, "sum_gate_second": sum_gate_second, "sum_up_second": sum_up_second, "sum_down_second": sum_down_second}


norm_eps = 1e-06

def normalize(values, gain_vector):
    widened = values.astype(jnp.float32)
    factor = lax.rsqrt(lax.optimization_barrier(jnp.mean(widened * widened, axis=-1, keepdims=True)) + norm_eps)
    normed = (widened * factor * gain_vector.astype(jnp.float32)).astype(jnp.bfloat16)
    return (widened, factor, normed)

def groupwise(operands, part_count):
    part_width = operands[0][0].shape[1] // part_count
    running = jnp.zeros((operands[0][0].shape[0], operands[0][1].shape[1]), jnp.float32)
    for part_index in range(part_count):
        lower = part_index * part_width
        product = jnp.zeros_like(running)
        for left_rows, right_cols in operands:
            product = product + jnp.dot(left_rows[:, lower:lower + part_width], right_cols[lower:lower + part_width], preferred_element_type=jnp.float32)
        rounded = lax.optimization_barrier(product.astype(jnp.bfloat16))
        running = running + rounded.astype(jnp.float32)
    return running

def block_forward(values, gain_vector, w_gate, w_up, w_down):
    widened, factor, normed = normalize(values, gain_vector)
    gate_pre = jnp.dot(normed, w_gate, preferred_element_type=jnp.float32)
    up_pre = jnp.dot(normed, w_up, preferred_element_type=jnp.float32)
    hidden = (jax.nn.silu(gate_pre) * up_pre).astype(jnp.bfloat16)
    branch = groupwise(((hidden, w_down),), N_TP)
    return (widened + 0.5 * branch).astype(jnp.bfloat16)

def block_backward(values, cotangent, gain_vector, w_gate, w_up, w_down):
    widened, factor, normed = normalize(values, gain_vector)
    gate_pre = jnp.dot(normed, w_gate, preferred_element_type=jnp.float32)
    up_pre = jnp.dot(normed, w_up, preferred_element_type=jnp.float32)
    sigmoid_gate = jax.nn.sigmoid(gate_pre)
    activated = gate_pre * sigmoid_gate
    hidden = (activated * up_pre).astype(jnp.bfloat16)
    hidden_grad = 0.5 * jnp.dot(cotangent, w_down.T, preferred_element_type=jnp.float32)
    gate_grad = (hidden_grad * up_pre * sigmoid_gate * (1.0 + gate_pre * (1.0 - sigmoid_gate))).astype(jnp.bfloat16)
    up_grad = (hidden_grad * activated).astype(jnp.bfloat16)
    normed_grad = groupwise(((gate_grad, w_gate.T), (up_grad, w_up.T)), N_TP)
    scaled = normed_grad * gain_vector.astype(jnp.float32)
    unit_rows = widened * factor
    rows_grad = cotangent.astype(jnp.float32) + factor * (scaled - unit_rows * lax.optimization_barrier(jnp.mean(scaled * unit_rows, axis=-1, keepdims=True)))
    grad_gate = jnp.dot(normed.T, gate_grad, preferred_element_type=jnp.float32)
    grad_up = jnp.dot(normed.T, up_grad, preferred_element_type=jnp.float32)
    grad_down = 0.5 * jnp.dot(hidden.T, cotangent, preferred_element_type=jnp.float32)
    return (rows_grad, (grad_gate, grad_up, grad_down))

def reference(late_input, early_input, early_mid, cotangent, gain_first, gain_second, gate_first, up_first, down_first, gate_second, up_second, down_second, sum_gate_first, sum_up_first, sum_down_first, sum_gate_second, sum_up_second, sum_down_second):
    late_mid = block_forward(late_input, gain_first, gate_first, up_first, down_first)
    late_out = block_forward(late_mid, gain_second, gate_second, up_second, down_second)
    mid_grad, grads_second = block_backward(early_mid, cotangent, gain_second, gate_second, up_second, down_second)
    mid_grad = mid_grad.astype(jnp.bfloat16)
    rows_grad, grads_first = block_backward(early_input, mid_grad, gain_first, gate_first, up_first, down_first)
    return (late_mid, late_out, rows_grad.astype(jnp.bfloat16), sum_gate_first + grads_first[0], sum_up_first + grads_first[1], sum_down_first + grads_first[2], sum_gate_second + grads_second[0], sum_up_second + grads_second[1], sum_down_second + grads_second[2])
```

```python
import jax
import jax.numpy as jnp
from jax import lax
from jax.sharding import PartitionSpec as P

norm_eps = 1e-06
H = 176


def normalize(values, gain_vector):
    widened = values.astype(jnp.float32)
    factor = lax.rsqrt(jnp.mean(widened * widened, axis=-1, keepdims=True) + norm_eps)
    normed = (widened * factor * gain_vector).astype(jnp.bfloat16)
    return (widened, factor, normed)


def dot_nn(a, b):
    return jnp.dot(a, b, preferred_element_type=jnp.float32)


def dot_nt(a, b):
    return lax.dot_general(a, b, (((1,), (1,)), ((), ())), preferred_element_type=jnp.float32)


def dot_tn(a, b):
    return lax.dot_general(a, b, (((0,), (0,)), ((), ())), preferred_element_type=jnp.float32)


def forward_partial(values, gain_vector, w_in, w_down):
    _, _, normed = normalize(values, gain_vector)
    pre = dot_nn(normed, w_in)
    hidden = (jax.nn.silu(pre[:, :H]) * pre[:, H:]).astype(jnp.bfloat16)
    return dot_nt(hidden, w_down).astype(jnp.bfloat16)


def backward_partial(values, cot, gain_vector, w_in, w_down):
    _, _, normed = normalize(values, gain_vector)
    pre = dot_nn(normed, w_in)
    gate_pre, up_pre = pre[:, :H], pre[:, H:]
    s = jax.nn.sigmoid(gate_pre)
    activated = gate_pre * s
    hidden = (activated * up_pre).astype(jnp.bfloat16)
    hidden_grad = 0.5 * dot_nn(cot, w_down)
    gate_grad = (hidden_grad * up_pre * s * (1.0 + gate_pre * (1.0 - s))).astype(jnp.bfloat16)
    up_grad = (hidden_grad * activated).astype(jnp.bfloat16)
    both = jnp.concatenate([gate_grad, up_grad], axis=1)
    partial_value = dot_nt(both, w_in).astype(jnp.bfloat16)
    return partial_value, (normed, both, hidden)


def weight_partial(normed, both, hidden, cot):
    in_part = dot_tn(normed, both)
    down_part = 0.5 * dot_tn(cot, hidden)
    return jnp.concatenate([in_part.astype(jnp.bfloat16), down_part.astype(jnp.bfloat16)], axis=1)


def spread_sum(first, second):
    n = lax.axis_size("tp")
    rows = first.shape[0] // n
    both = jnp.stack([first.reshape(n, rows, -1), second.reshape(n, rows, -1)], axis=1)
    got = lax.all_to_all(both, "tp", split_axis=0, concat_axis=0, tiled=True)
    total = jnp.sum(got.astype(jnp.float32), axis=0)
    return total[0], total[1]


def share_rows(first, second):
    n = lax.axis_size("tp")
    both = jnp.stack([first, second], axis=0)
    out = jnp.broadcast_to(both[None], (n,) + both.shape)
    got = lax.all_to_all(out, "tp", split_axis=0, concat_axis=0, tiled=True)
    return got[:, 0].reshape(-1, both.shape[-1]), got[:, 1].reshape(-1, both.shape[-1])


def own_rows(a):
    rows = a.shape[0] // lax.axis_size("tp")
    return lax.dynamic_slice_in_dim(a, lax.axis_index("tp") * rows, rows, axis=0)


def forward_rows(values, branch):
    return (values.astype(jnp.float32) + 0.5 * branch).astype(jnp.bfloat16)


def backward_rows(values, cot, gain_vector, normed_grad):
    widened = values.astype(jnp.float32)
    factor = lax.rsqrt(jnp.mean(widened * widened, axis=-1, keepdims=True) + norm_eps)
    scaled = normed_grad * gain_vector
    unit_rows = widened * factor
    rows_grad = cot.astype(jnp.float32) + factor * (
        scaled - unit_rows * jnp.mean(scaled * unit_rows, axis=-1, keepdims=True)
    )
    return rows_grad.astype(jnp.bfloat16)


def per_device(
    late_input,
    early_input,
    early_mid,
    cotangent,
    gain_first,
    gain_second,
    gate_first,
    up_first,
    down_first,
    gate_second,
    up_second,
    down_second,
    sum_gate_first,
    sum_up_first,
    sum_down_first,
    sum_gate_second,
    sum_up_second,
    sum_down_second,
):
    packed = jnp.concatenate(
        [gate_first, up_first, down_first.T, gate_second, up_second, down_second.T], axis=1
    )
    whole = lax.all_gather(packed, "fs", axis=0, tiled=True)
    in_first, down_t_first = whole[:, : 2 * H], whole[:, 2 * H : 3 * H]
    in_second, down_t_second = whole[:, 3 * H : 5 * H], whole[:, 5 * H :]

    part_f = forward_partial(late_input, gain_first, in_first, down_t_first)
    part_b, saved_second = backward_partial(
        early_mid, cotangent, gain_second, in_second, down_t_second
    )
    grad_second = lax.psum_scatter(
        weight_partial(*saved_second, cotangent), "fs", scatter_dimension=0, tiled=True
    )
    sum_f, sum_b = spread_sum(part_f, part_b)
    late_mid, mid_grad = share_rows(
        forward_rows(own_rows(late_input), sum_f),
        backward_rows(own_rows(early_mid), own_rows(cotangent), gain_second, sum_b),
    )

    part_f2 = forward_partial(late_mid, gain_second, in_second, down_t_second)
    part_b2, saved_first = backward_partial(
        early_input, mid_grad, gain_first, in_first, down_t_first
    )
    grad_first = lax.psum_scatter(
        weight_partial(*saved_first, mid_grad), "fs", scatter_dimension=0, tiled=True
    )
    sum_f2, sum_b2 = spread_sum(part_f2, part_b2)
    late_out, input_grad = share_rows(
        forward_rows(own_rows(late_mid), sum_f2),
        backward_rows(own_rows(early_input), own_rows(mid_grad), gain_first, sum_b2),
    )
    g1 = grad_first.astype(jnp.float32)
    g2 = grad_second.astype(jnp.float32)
    return (
        late_mid,
        late_out,
        input_grad,
        sum_gate_first + g1[:, :H],
        sum_up_first + g1[:, H : 2 * H],
        sum_down_first + g1[:, 2 * H :].T,
        sum_gate_second + g2[:, :H],
        sum_up_second + g2[:, H : 2 * H],
        sum_down_second + g2[:, 2 * H :].T,
    )


def solution(mesh):
    rows, w_in, w_out = P("fs", None), P("fs", "tp"), P("tp", "fs")
    weights = (w_in, w_in, w_out) * 2
    return jax.shard_map(
        per_device,
        mesh=mesh,
        in_specs=(rows,) * 4 + (P(), P()) + weights + weights,
        out_specs=(rows,) * 3 + weights,
        check_vma=False,
    )
```

```python
import jax
import jax.numpy as jnp
from jax import lax
from jax.sharding import PartitionSpec as P

norm_eps = 1e-06
H = 176


def normalize(values, gain_vector):
    widened = values.astype(jnp.float32)
    factor = lax.rsqrt(jnp.mean(widened * widened, axis=-1, keepdims=True) + norm_eps)
    normed = (widened * factor * gain_vector).astype(jnp.bfloat16)
    return (widened, factor, normed)


def dot_nn(a, b):
    return jnp.dot(a, b, preferred_element_type=jnp.float32)


def dot_nt(a, b):
    return lax.dot_general(a, b, (((1,), (1,)), ((), ())), preferred_element_type=jnp.float32)


def dot_tn(a, b):
    return lax.dot_general(a, b, (((0,), (0,)), ((), ())), preferred_element_type=jnp.float32)


def forward_partial(values, gain_vector, w_in, w_down):
    _, _, normed = normalize(values, gain_vector)
    pre = dot_nn(normed, w_in)
    hidden = (jax.nn.silu(pre[:, :H]) * pre[:, H:]).astype(jnp.bfloat16)
    return dot_nt(hidden, w_down).astype(jnp.bfloat16)


def backward_partial(values, cot, gain_vector, w_in, w_down):
    _, _, normed = normalize(values, gain_vector)
    pre = dot_nn(normed, w_in)
    gate_pre, up_pre = pre[:, :H], pre[:, H:]
    s = jax.nn.sigmoid(gate_pre)
    activated = gate_pre * s
    hidden = (activated * up_pre).astype(jnp.bfloat16)
    hidden_grad = 0.5 * dot_nn(cot, w_down)
    gate_grad = (hidden_grad * up_pre * s * (1.0 + gate_pre * (1.0 - s))).astype(jnp.bfloat16)
    up_grad = (hidden_grad * activated).astype(jnp.bfloat16)
    both = jnp.concatenate([gate_grad, up_grad], axis=1)
    partial_value = dot_nt(both, w_in).astype(jnp.bfloat16)
    return partial_value, (normed, both, hidden)


def weight_partial(normed, both, hidden, cot):
    in_part = dot_tn(normed, both)
    down_part = 0.5 * dot_tn(cot, hidden)
    return jnp.concatenate([in_part.astype(jnp.bfloat16), down_part.astype(jnp.bfloat16)], axis=1)


def spread_sum(first, second):
    n = lax.axis_size("tp")
    rows = first.shape[0] // n
    both = jnp.stack([first.reshape(n, rows, -1), second.reshape(n, rows, -1)], axis=1)
    got = lax.all_to_all(both, "tp", split_axis=0, concat_axis=0, tiled=True)
    total = jnp.sum(got.astype(jnp.float32), axis=0)
    return total[0], total[1]


def share_rows(first, second):
    n = lax.axis_size("tp")
    both = jnp.stack([first, second], axis=0)
    out = jnp.broadcast_to(both[None], (n,) + both.shape)
    got = lax.all_to_all(out, "tp", split_axis=0, concat_axis=0, tiled=True)
    return got[:, 0].reshape(-1, both.shape[-1]), got[:, 1].reshape(-1, both.shape[-1])


def own_rows(a):
    rows = a.shape[0] // lax.axis_size("tp")
    return lax.dynamic_slice_in_dim(a, lax.axis_index("tp") * rows, rows, axis=0)


def moved(a, step):
    n = lax.axis_size("fs")
    return lax.ppermute(a, "fs", [(q, (q + 2 * step) % n) for q in range(n)])


def reduce_blocks(g):
    n = lax.axis_size("fs")
    index = lax.axis_index("fs")
    core, z = index % 2, index // 2
    rows, cols = g.shape[0] // n, g.shape[1]
    f32 = jnp.float32

    def take(a, k):
        return lax.dynamic_index_in_dim(a, k, 0, keepdims=False)

    blocks = g.reshape(n // 8, 4, 2, rows, cols)
    mine = lax.dynamic_index_in_dim(blocks, core, 2, keepdims=False)
    theirs = lax.dynamic_index_in_dim(blocks, 1 - core, 2, keepdims=False)
    got = lax.ppermute(theirs, "fs", [(q, q ^ 1) for q in range(n)])
    pair = (mine.astype(f32) + got.astype(f32)).astype(jnp.bfloat16)

    def of_class(k):
        return lax.dynamic_index_in_dim(pair, (z + k) % 4, 1, keepdims=False)

    half = rows // 2
    far_class = of_class(2)
    near = (
        moved(far_class[:, :half], -2),
        moved(far_class[:, half:], 2),
        moved(of_class(1), 1),
        moved(of_class(3), -1),
    )
    quad = (
        of_class(0).astype(f32)
        + near[2].astype(f32)
        + near[3].astype(f32)
        + jnp.concatenate([near[0], near[1]], axis=1).astype(f32)
    ).astype(jnp.bfloat16)
    kz = z // 4
    far = (
        moved(take(quad, (kz + 2) % 4), 8),
        moved(take(quad, (kz + 1) % 4), 4),
        moved(take(quad, (kz + 3) % 4), -4),
    )
    return take(quad, kz).astype(f32) + far[0].astype(f32) + far[1].astype(f32) + far[2].astype(f32)


def forward_rows(values, branch):
    return (values.astype(jnp.float32) + 0.5 * branch).astype(jnp.bfloat16)


def backward_rows(values, cot, gain_vector, normed_grad):
    widened = values.astype(jnp.float32)
    factor = lax.rsqrt(jnp.mean(widened * widened, axis=-1, keepdims=True) + norm_eps)
    scaled = normed_grad * gain_vector
    unit_rows = widened * factor
    rows_grad = cot.astype(jnp.float32) + factor * (
        scaled - unit_rows * jnp.mean(scaled * unit_rows, axis=-1, keepdims=True)
    )
    return rows_grad.astype(jnp.bfloat16)


def per_device(
    late_input,
    early_input,
    early_mid,
    cotangent,
    gain_first,
    gain_second,
    gate_first,
    up_first,
    down_first,
    gate_second,
    up_second,
    down_second,
    sum_gate_first,
    sum_up_first,
    sum_down_first,
    sum_gate_second,
    sum_up_second,
    sum_down_second,
):
    packed = jnp.concatenate(
        [gate_first, up_first, down_first.T, gate_second, up_second, down_second.T], axis=1
    )
    whole = lax.all_gather(packed, "fs", axis=0, tiled=True)
    in_first, down_t_first = whole[:, : 2 * H], whole[:, 2 * H : 3 * H]
    in_second, down_t_second = whole[:, 3 * H : 5 * H], whole[:, 5 * H :]

    part_f = forward_partial(late_input, gain_first, in_first, down_t_first)
    part_b, saved_second = backward_partial(
        early_mid, cotangent, gain_second, in_second, down_t_second
    )
    grad_second = lax.psum_scatter(
        weight_partial(*saved_second, cotangent), "fs", scatter_dimension=0, tiled=True
    )
    sum_f, sum_b = spread_sum(part_f, part_b)
    late_mid, mid_grad = share_rows(
        forward_rows(own_rows(late_input), sum_f),
        backward_rows(own_rows(early_mid), own_rows(cotangent), gain_second, sum_b),
    )

    part_f2 = forward_partial(late_mid, gain_second, in_second, down_t_second)
    part_b2, saved_first = backward_partial(
        early_input, mid_grad, gain_first, in_first, down_t_first
    )
    g1 = reduce_blocks(weight_partial(*saved_first, mid_grad))
    sum_f2, sum_b2 = spread_sum(part_f2, part_b2)
    late_out, input_grad = share_rows(
        forward_rows(own_rows(late_mid), sum_f2),
        backward_rows(own_rows(early_input), own_rows(mid_grad), gain_first, sum_b2),
    )
    g2 = grad_second.astype(jnp.float32)
    return (
        late_mid,
        late_out,
        input_grad,
        sum_gate_first + g1[:, :H],
        sum_up_first + g1[:, H : 2 * H],
        sum_down_first + g1[:, 2 * H :].T,
        sum_gate_second + g2[:, :H],
        sum_up_second + g2[:, H : 2 * H],
        sum_down_second + g2[:, 2 * H :].T,
    )


def solution(mesh):
    rows, w_in, w_out = P("fs", None), P("fs", "tp"), P("tp", "fs")
    weights = (w_in, w_in, w_out) * 2
    return jax.shard_map(
        per_device,
        mesh=mesh,
        in_specs=(rows,) * 4 + (P(), P()) + weights + weights,
        out_specs=(rows,) * 3 + weights,
        check_vma=False,
    )
```

```python
import jax
import jax.numpy as jnp
from jax import lax
from jax.experimental import pallas as pl
from jax.experimental.pallas import tpu as pltpu
from jax.sharding import PartitionSpec as P

norm_eps = 1e-06
f32, bf16 = jnp.float32, jnp.bfloat16


def dot_nn(a, b):
    return jnp.dot(a, b, preferred_element_type=f32)


def dot_nt(a, b):
    return lax.dot_general(a, b, (((1,), (1,)), ((), ())), preferred_element_type=f32)


def dot_tn(a, b):
    return lax.dot_general(a, b, (((0,), (0,)), ((), ())), preferred_element_type=f32)


def row_factor(widened):
    return lax.rsqrt(jnp.mean(widened * widened, axis=-1, keepdims=True) + norm_eps)


def normalize(values, gain):
    widened = values.astype(f32)
    return (widened * row_factor(widened) * gain).astype(bf16)


def widen_cols(a, width):
    return jnp.concatenate([a, jnp.zeros((a.shape[0], width - a.shape[1]), a.dtype)], axis=1)


def forward_part(normed, w_in, w_down, h):
    pre = dot_nn(normed, w_in)
    gate, up = pre[:, :h], pre[:, h : 2 * h]
    hidden = (gate * jax.nn.sigmoid(gate) * up).astype(bf16)
    return dot_nt(widen_cols(hidden, w_down.shape[1]), w_down)


def backward_part(pre, cot, w_in, w_down, h):
    gate, up = pre[:, :h], pre[:, h : 2 * h]
    s = jax.nn.sigmoid(gate)
    activated = gate * s
    hidden = (activated * up).astype(bf16)
    hidden_grad = 0.5 * dot_nn(cot, w_down)[:, :h]
    gate_grad = hidden_grad * up * s * (1.0 + gate * (1.0 - s))
    both = jnp.concatenate([gate_grad, hidden_grad * activated], axis=1).astype(bf16)
    return dot_nt(widen_cols(both, w_in.shape[1]), w_in), both, hidden


def put_rows(send, part, half):
    n, rows = send.shape[0], send.shape[1] // 2
    for t in range(n):
        send[t, half * rows : (half + 1) * rows, :] = part[t * rows : (t + 1) * rows].astype(bf16)


def columns(w, h):
    wide, narrow = padded(2 * h), padded(h)
    block = wide + narrow
    return tuple(
        (slice(k * block, k * block + wide), slice(k * block + wide, (k + 1) * block))
        for k in range(2)
    )


def padded(n):
    return -(-n // 128) * 128


def stage_one(h, late, early, cot, gain_1, gain_2, w, send, normed, both, hidden):
    (in_1, down_1), (in_2, down_2) = columns(w, h)
    put_rows(send, forward_part(normalize(late[...], gain_1[...]), w[:, in_1], w[:, down_1], h), 0)
    rows = normalize(early[...], gain_2[...])
    normed[...] = rows
    part, both[...], hidden[...] = backward_part(
        dot_nn(rows, w[:, in_2]), cot[...], w[:, in_2], w[:, down_2], h
    )
    put_rows(send, part, 1)


def stage_two(h, got, early, gain_1, gain_2, w, late, cot, send, normed, both, hidden):
    (in_1, down_1), (in_2, down_2) = columns(w, h)
    rows = got.shape[1] // 2
    for t in range(got.shape[0]):
        late[t * rows : (t + 1) * rows, :] = got[t, :rows, :]
        cot[t * rows : (t + 1) * rows, :] = got[t, rows:, :]
    saved = normalize(early[...], gain_1[...])
    normed[...] = saved
    part, both[...], hidden[...] = backward_part(
        dot_nn(saved, w[:, in_1]), cot[...], w[:, in_1], w[:, down_1], h
    )
    put_rows(send, part, 1)
    put_rows(send, forward_part(normalize(late[...], gain_2[...]), w[:, in_2], w[:, down_2], h), 0)


def update_rows(got, late, early, cot, gain, out, own):
    n, rows = got.shape[0], got.shape[1] // 2
    total = got[0].astype(f32)
    for t in range(1, n):
        total = total + got[t].astype(f32)
    own[:rows, :] = (late[...].astype(f32) + 0.5 * total[:rows]).astype(bf16)
    widened = early[...].astype(f32)
    factor = row_factor(widened)
    scaled = total[rows:] * gain[...]
    unit = widened * factor
    own[rows:, :] = (
        cot[...].astype(f32)
        + factor * (scaled - unit * jnp.mean(scaled * unit, axis=-1, keepdims=True))
    ).astype(bf16)
    for t in range(n):
        out[t] = own[...]


def block_products(normed, both, hidden, cot, z, size):
    cols = slice(z * size, (z + 1) * size)
    return dot_tn(normed[:, cols], both[...]), 0.5 * dot_tn(cot[:, cols], hidden[...])


def weight_parts(normed, both, hidden, cot, out):
    size, wide = 128, both.shape[1]
    for z in range(normed.shape[1] // size):
        ins, downs = block_products(normed, both, hidden, cot, z, size)
        out[z * size : (z + 1) * size, :wide] = ins.astype(bf16)
        out[z * size : (z + 1) * size, wide:] = downs.astype(bf16)


def weight_parts_by_core(core, normed, both, hidden, cot, mine, theirs):
    rows, wide = mine.shape[1], both.shape[1]
    first = core[0] == 0
    for z in range(mine.shape[0]):
        for part, cols in zip(
            block_products(normed, both, hidden, cot, z, 2 * rows),
            (slice(0, wide), slice(wide, mine.shape[2])),
        ):
            top, bottom = part[:rows], part[rows:]
            mine[z, :, cols] = jnp.where(first, top, bottom).astype(bf16)
            theirs[z, :, cols] = jnp.where(first, bottom, top).astype(bf16)


def call(body, outs, *args, scalars=0):
    spaces = [pl.BlockSpec(memory_space=pltpu.SMEM)] * scalars
    spaces += [pl.BlockSpec(memory_space=pltpu.VMEM)] * (len(args) - scalars)
    return pl.pallas_call(
        body,
        in_specs=spaces,
        out_specs=[pl.BlockSpec(memory_space=pltpu.VMEM)] * len(outs),
        out_shape=[jax.ShapeDtypeStruct(shape, bf16) for shape in outs],
        compiler_params=pltpu.CompilerParams(vmem_limit_bytes=48 * 2**20),
    )(*args)


def own_rows(a):
    rows = a.shape[0] // lax.axis_size("tp")
    return lax.dynamic_slice_in_dim(a, lax.axis_index("tp") * rows, rows, axis=0)


def exchange(a):
    return lax.all_to_all(a, "tp", split_axis=0, concat_axis=0, tiled=True)


def moved(a, step):
    n = lax.axis_size("fs")
    return lax.ppermute(a, "fs", [(q, (q + 2 * step) % n) for q in range(n)])


def swapped(a):
    n = lax.axis_size("fs")
    return lax.ppermute(a, "fs", [(q, q ^ 1) for q in range(n)])


def pick(a, k, axis):
    return lax.dynamic_index_in_dim(a, k, axis, keepdims=False)


def reduce_blocks(mine, theirs):
    z = lax.axis_index("fs") // 2
    pair = (mine.astype(f32) + swapped(theirs).astype(f32)).astype(bf16)
    pair = pair.reshape(pair.shape[0] // 4, 4, *pair.shape[1:])

    def of_class(k):
        return pick(pair, (z + k) % 4, 1)

    half = pair.shape[2] // 2
    across = of_class(2)
    left = moved(of_class(1), 1)
    right = moved(of_class(3), -1)
    top = moved(across[:, :half], -2)
    bottom = moved(across[:, half:], 2)
    quad = (
        of_class(0).astype(f32)
        + left.astype(f32)
        + right.astype(f32)
        + jnp.concatenate([top, bottom], axis=1).astype(f32)
    ).astype(bf16)
    kz = z // 4
    far = (
        moved(pick(quad, (kz + 1) % 4, 0), 4),
        moved(pick(quad, (kz + 3) % 4, 0), -4),
        moved(pick(quad, (kz + 2) % 4, 0), 8),
    )
    return pick(quad, kz, 0).astype(f32) + sum(a.astype(f32) for a in far)


def per_device(
    late_input,
    early_input,
    early_mid,
    cotangent,
    gain_first,
    gain_second,
    gate_first,
    up_first,
    down_first,
    gate_second,
    up_second,
    down_second,
    sum_gate_first,
    sum_up_first,
    sum_down_first,
    sum_gate_second,
    sum_up_second,
    sum_down_second,
):
    h = gate_first.shape[1]
    tokens, d = late_input.shape
    n = lax.axis_size("tp")
    n_fs = lax.axis_size("fs")
    gain_1, gain_2 = gain_first[None], gain_second[None]
    wide = (padded(2 * h) - 2 * h, padded(h) - h)
    packed = jnp.concatenate(
        [
            jnp.pad(gate_first, ((0, 0), (0, 0))),
            jnp.pad(up_first, ((0, 0), (0, wide[0]))),
            jnp.pad(down_first.T, ((0, 0), (0, wide[1]))),
            jnp.pad(gate_second, ((0, 0), (0, 0))),
            jnp.pad(up_second, ((0, 0), (0, wide[0]))),
            jnp.pad(down_second.T, ((0, 0), (0, wide[1]))),
        ],
        axis=1,
    )
    w = lax.all_gather(packed, "fs", axis=0, tiled=True)
    core = (lax.axis_index("fs") % 2)[None].astype(jnp.int32)

    spread = (n, 2 * (tokens // n), d)
    saved_shapes = ((tokens, d), (tokens, 2 * h), (tokens, h))
    own = (2 * (tokens // n), d)
    send, *saved_second = call(
        lambda *refs: stage_one(h, *refs), (spread,) + saved_shapes,
        late_input, early_mid, cotangent, gain_1, gain_2, w,
    )
    got = exchange(send)
    (parts_second,) = call(weight_parts, ((d, 3 * h),), *saved_second, cotangent)
    grad_second = lax.psum_scatter(parts_second, "fs", scatter_dimension=0, tiled=True)
    got, _ = lax.optimization_barrier((got, parts_second))
    send, rows = call(
        update_rows, (spread, own),
        got, own_rows(late_input), own_rows(early_mid), own_rows(cotangent), gain_2,
    )
    got = exchange(send)
    late_mid, mid_grad, send, *saved_first = call(
        lambda *refs: stage_two(h, *refs), ((tokens, d), (tokens, d), spread) + saved_shapes,
        got, early_input, gain_1, gain_2, w,
    )
    got = exchange(send)
    by_core = (n_fs // 2, d // n_fs, 3 * h)
    mine, theirs = call(
        weight_parts_by_core, (by_core, by_core), core, *saved_first, mid_grad, scalars=1
    )
    g1 = reduce_blocks(mine, theirs)
    half = tokens // n
    send, _ = call(
        update_rows, (spread, own),
        got, rows[:half], own_rows(early_input), rows[half:], gain_1,
    )
    got = exchange(send)
    late_out = got[:, :half].reshape(tokens, d)
    input_grad = got[:, half:].reshape(tokens, d)
    g2 = grad_second.astype(f32)
    return (
        late_mid,
        late_out,
        input_grad,
        sum_gate_first + g1[:, :h],
        sum_up_first + g1[:, h : 2 * h],
        sum_down_first + g1[:, 2 * h :].T,
        sum_gate_second + g2[:, :h],
        sum_up_second + g2[:, h : 2 * h],
        sum_down_second + g2[:, 2 * h :].T,
    )


def solution(mesh):
    rows, w_in, w_out = P("fs", None), P("fs", "tp"), P("tp", "fs")
    weights = (w_in, w_in, w_out) * 2
    return jax.shard_map(
        per_device,
        mesh=mesh,
        in_specs=(rows,) * 4 + (P(), P()) + weights + weights,
        out_specs=(rows,) * 3 + weights,
        check_vma=False,
    )
```

```python
import jax
import jax.numpy as jnp
from jax import lax
from jax.experimental import pallas as pl
from jax.experimental.pallas import tpu as pltpu
from jax.sharding import PartitionSpec as P

norm_eps = 1e-06
f32, bf16 = jnp.float32, jnp.bfloat16


def dot_nn(a, b):
    return jnp.dot(a, b, preferred_element_type=f32)


def dot_nt(a, b):
    return lax.dot_general(a, b, (((1,), (1,)), ((), ())), preferred_element_type=f32)


def dot_tn(a, b):
    return lax.dot_general(a, b, (((0,), (0,)), ((), ())), preferred_element_type=f32)


def row_factor(widened):
    return lax.rsqrt(jnp.mean(widened * widened, axis=-1, keepdims=True) + norm_eps)


def normalize(values, gain):
    widened = values.astype(f32)
    return (widened * row_factor(widened) * gain).astype(bf16)


def widen_cols(a, width):
    return jnp.concatenate([a, jnp.zeros((a.shape[0], width - a.shape[1]), a.dtype)], axis=1)


def forward_part(normed, w_in, w_down, h):
    pre = dot_nn(normed, w_in)
    gate, up = pre[:, :h], pre[:, h : 2 * h]
    hidden = (gate * jax.nn.sigmoid(gate) * up).astype(bf16)
    return dot_nt(widen_cols(hidden, w_down.shape[1]), w_down)


def backward_part(pre, cot, w_in, w_down, h):
    gate, up = pre[:, :h], pre[:, h : 2 * h]
    s = jax.nn.sigmoid(gate)
    activated = gate * s
    hidden = (activated * up).astype(bf16)
    hidden_grad = 0.5 * dot_nn(cot, w_down)[:, :h]
    gate_grad = hidden_grad * up * s * (1.0 + gate * (1.0 - s))
    both = jnp.concatenate([gate_grad, hidden_grad * activated], axis=1).astype(bf16)
    return dot_nt(widen_cols(both, w_in.shape[1]), w_in), both, hidden


def put_rows(send, part, at):
    rows = part.shape[0] // send.shape[0]
    for t in range(send.shape[0]):
        send[t, at : at + rows, :] = part[t * rows : (t + 1) * rows].astype(bf16)


def get_rows(whole, got, at):
    rows = whole.shape[0] // got.shape[0]
    for t in range(got.shape[0]):
        whole[t * rows : (t + 1) * rows, :] = got[t, at : at + rows, :]


def padded(n):
    return -(-n // 128) * 128


def sum_rows(got, at, rows):
    total = got[0, at : at + rows, :].astype(f32)
    for t in range(1, got.shape[0]):
        total = total + got[t, at : at + rows, :].astype(f32)
    return total


def forward_rows(late, branch):
    return (late.astype(f32) + 0.5 * branch).astype(bf16)


def backward_rows(early, cot, gain, normed_grad):
    widened = early.astype(f32)
    factor = row_factor(widened)
    scaled = normed_grad * gain
    unit = widened * factor
    mean = jnp.mean(scaled * unit, axis=-1, keepdims=True)
    return (cot.astype(f32) + factor * (scaled - unit * mean)).astype(bf16)


def backward_second(h, early, cot, gain, w, send, normed, both, hidden):
    split = padded(2 * h)
    rows = normalize(early[...], gain[...])
    normed[...] = rows
    part, both[...], hidden[...] = backward_part(
        dot_nn(rows, w[:, :split]), cot[...], w[:, :split], w[:, split:], h
    )
    put_rows(send, part, 0)


def backward_first(h, got, early, gain, w, send, normed, both, hidden, cot):
    get_rows(cot, got, 0)
    backward_second(h, early, cot, gain, w, send, normed, both, hidden)


def forward_first(h, late, gain, w, send):
    split = padded(2 * h)
    part = forward_part(normalize(late[...], gain[...]), w[:, :split], w[:, split:], h)
    put_rows(send, part, 0)


def rows_b(got, early, cot, gain, send, own):
    own[...] = backward_rows(early[...], cot[...], gain[...], sum_rows(got, 0, own.shape[0]))
    for t in range(send.shape[0]):
        send[t] = own[...]


def rows_f(got, late, other, send, own):
    rows = own.shape[0]
    own[...] = forward_rows(late[...], sum_rows(got, 0, rows))
    for t in range(send.shape[0]):
        send[t, :rows, :] = own[...]
        send[t, rows:, :] = other[t]


def middle(h, got, early, cot, gain_1, gain_2, w, send, late):
    rows = early.shape[0]
    get_rows(late, got, 0)
    split = padded(2 * h)
    part = forward_part(normalize(late[...], gain_2[...]), w[:, :split], w[:, split:], h)
    put_rows(send, part, 0)
    grad = backward_rows(early[...], cot[...], gain_1[...], sum_rows(got, rows, rows))
    for t in range(send.shape[0]):
        send[t, rows:, :] = grad


def last_rows(got, late, send, grad):
    rows = late.shape[0]
    out = forward_rows(late[...], sum_rows(got, 0, rows))
    get_rows(grad, got, rows)
    for t in range(send.shape[0]):
        send[t] = out


def near_parts(place, mine, got, own, right, left, top, bottom):
    half = top.shape[1]
    for k in range(own.shape[0]):
        for step in range(4):
            at = 4 * k + lax.rem(place[0] + step, 4)
            pair = (mine[at].astype(f32) + got[at].astype(f32)).astype(bf16)
            if step == 2:
                top[k] = pair[:half]
                bottom[k] = pair[half:]
            else:
                {0: own, 1: right, 3: left}[step][k] = pair


def far_parts(place, *refs):
    outs, scratch = refs[10:14], refs[14]
    for block in range(2):
        own, top, bottom, right, left = refs[5 * block : 5 * block + 5]
        half = top.shape[1]
        for k in range(own.shape[0]):
            total = own[k].astype(f32) + right[k].astype(f32) + left[k].astype(f32)
            scratch[k, :half] = (total[:half] + top[k].astype(f32)).astype(bf16)
            scratch[k, half:] = (total[half:] + bottom[k].astype(f32)).astype(bf16)
        for step in range(4):
            outs[step][block] = scratch[lax.rem(place[0] + step, 4)]


def block_products(normed, both, hidden, cot, z, size):
    cols = slice(z * size, (z + 1) * size)
    return dot_tn(normed[:, cols], both[...]), 0.5 * dot_tn(cot[:, cols], hidden[...])


def weight_parts_by_core(core, normed, both, hidden, cot, mine, theirs):
    rows, wide = mine.shape[1], both.shape[1]
    first = core[0] == 0
    for z in range(mine.shape[0]):
        for part, cols in zip(
            block_products(normed, both, hidden, cot, z, 2 * rows),
            (slice(0, wide), slice(wide, mine.shape[2])),
        ):
            top, bottom = part[:rows], part[rows:]
            mine[z, :, cols] = jnp.where(first, top, bottom).astype(bf16)
            theirs[z, :, cols] = jnp.where(first, bottom, top).astype(bf16)


def call(body, outs, *args, scalars=0, scratch=()):
    spaces = [pl.BlockSpec(memory_space=pltpu.SMEM)] * scalars
    spaces += [pl.BlockSpec(memory_space=pltpu.VMEM)] * (len(args) - scalars)
    return pl.pallas_call(
        body,
        in_specs=spaces,
        out_specs=[pl.BlockSpec(memory_space=pltpu.VMEM)] * len(outs),
        out_shape=[jax.ShapeDtypeStruct(shape, bf16) for shape in outs],
        scratch_shapes=[pltpu.VMEM(shape, bf16) for shape in scratch],
        compiler_params=pltpu.CompilerParams(vmem_limit_bytes=48 * 2**20),
    )(*args)


def own_rows(a):
    rows = a.shape[0] // lax.axis_size("tp")
    return lax.dynamic_slice_in_dim(a, lax.axis_index("tp") * rows, rows, axis=0)


def exchange(a):
    return lax.all_to_all(a, "tp", split_axis=0, concat_axis=0, tiled=True)


def moved(a, step):
    n = lax.axis_size("fs")
    return lax.ppermute(a, "fs", [(q, (q + 2 * step) % n) for q in range(n)])


def swapped(a):
    n = lax.axis_size("fs")
    return lax.ppermute(a, "fs", [(q, q ^ 1) for q in range(n)])


def far_groups():
    n = lax.axis_size("fs")
    return [[2 * z + c for z in range(r, n // 2, 4)] for r in range(4) for c in range(2)]


def gather_blocks(w):
    index = lax.axis_index("fs")
    core, z = index % 2, index // 2
    quad = lax.all_to_all(
        jnp.broadcast_to(w[None], (4,) + w.shape), "fs",
        split_axis=0, concat_axis=0, tiled=True, axis_index_groups=far_groups(),
    )
    half = w.shape[0] // 2
    right = moved(quad, -1)
    left = moved(quad, 1)
    top = moved(quad[:, :half], -2)
    bottom = moved(quad[:, half:], 2)
    own = jnp.stack([quad, right, jnp.concatenate([top, bottom], axis=1), left], axis=1)
    other = swapped(own)
    both = jnp.stack(
        [jnp.where(core == 0, own, other), jnp.where(core == 0, other, own)], axis=2
    )
    twice = jnp.concatenate([both, both], axis=1)
    turned = lax.dynamic_slice_in_dim(twice, (4 - z % 4) % 4, 4, axis=1)
    return turned.reshape(-1, w.shape[1])


def near_level(core, z, saved, cot, n_fs, d, h):
    block = (n_fs // 2, d // n_fs, 3 * h)
    mine, theirs = call(weight_parts_by_core, (block, block), core, *saved, cot, scalars=1)
    quarter = (4,) + block[1:]
    half = (4, block[1] // 2, block[2])
    got = swapped(theirs)
    own, right, left, top, bottom = call(
        near_parts, (quarter,) * 3 + (half,) * 2, z, mine, got, scalars=1
    )
    return own, moved(top, -2), moved(bottom, 2), moved(right, 1), moved(left, -1)


def far_level(kz, *parts):
    block = parts[0].shape
    outs = call(
        far_parts, ((2,) + block[1:],) * 4, kz, *parts, scalars=1, scratch=(block,)
    )
    across = moved(outs[2], 8)
    up, down = moved(outs[1], 4), moved(outs[3], -4)
    return outs[0].astype(f32) + up.astype(f32) + down.astype(f32) + across.astype(f32)


def pack(gate, up, down):
    h = gate.shape[1]
    return jnp.concatenate(
        [
            gate,
            jnp.pad(up, ((0, 0), (0, padded(2 * h) - 2 * h))),
            jnp.pad(down.T, ((0, 0), (0, padded(h) - h))),
        ],
        axis=1,
    )


def per_device(
    late_input,
    early_input,
    early_mid,
    cotangent,
    gain_first,
    gain_second,
    gate_first,
    up_first,
    down_first,
    gate_second,
    up_second,
    down_second,
    sum_gate_first,
    sum_up_first,
    sum_down_first,
    sum_gate_second,
    sum_up_second,
    sum_down_second,
):
    h = gate_first.shape[1]
    tokens, d = late_input.shape
    n = lax.axis_size("tp")
    n_fs = lax.axis_size("fs")
    rows = tokens // n
    gain_1, gain_2 = gain_first[None], gain_second[None]
    index = lax.axis_index("fs").astype(jnp.int32)
    core, z, kz = ((i.astype(jnp.int32))[None] for i in (index % 2, index // 2 % 4, index // 8))
    late_own, early_own, mid_own, cot_own = (
        own_rows(a) for a in (late_input, early_input, early_mid, cotangent)
    )
    w_2 = gather_blocks(pack(gate_second, up_second, down_second))
    w_1 = lax.all_gather(pack(gate_first, up_first, down_first), "fs", axis=0, tiled=True)

    single, double = (n, rows, d), (n, 2 * rows, d)
    saved_shapes = ((tokens, d), (tokens, 2 * h), (tokens, h))
    send, *saved_second = call(
        lambda *refs: backward_second(h, *refs), (single,) + saved_shapes,
        early_mid, cotangent, gain_2, w_2,
    )
    got = exchange(send)
    send, mid_rows = call(rows_b, (single, (rows, d)), got, mid_own, cot_own, gain_2)
    got_b = exchange(send)
    near_2 = near_level(core, z, saved_second, cotangent, n_fs, d, h)

    (send,) = call(
        lambda *refs: forward_first(h, *refs), (single,), late_input, gain_1, w_1
    )
    got_f = exchange(send)
    send_b, *saved_first, mid_grad = call(
        lambda *refs: backward_first(h, *refs), (single,) + saved_shapes + ((tokens, d),),
        got_b, early_input, gain_1, w_1,
    )
    send, late_rows = call(rows_f, (double, (rows, d)), got_f, late_own, send_b)
    got = exchange(send)
    near_1 = near_level(core, z, saved_first, mid_grad, n_fs, d, h)

    send, late_mid = call(
        lambda *refs: middle(h, *refs), (double, (tokens, d)),
        got, early_own, mid_rows, gain_1, gain_2, w_2,
    )
    got = exchange(send)
    g2, g1 = far_level(kz, *near_2, *near_1)
    send, input_grad = call(last_rows, (single, (tokens, d)), got, late_rows)
    late_out = exchange(send).reshape(tokens, d)
    return (
        late_mid,
        late_out,
        input_grad,
        sum_gate_first + g1[:, :h],
        sum_up_first + g1[:, h : 2 * h],
        sum_down_first + g1[:, 2 * h :].T,
        sum_gate_second + g2[:, :h],
        sum_up_second + g2[:, h : 2 * h],
        sum_down_second + g2[:, 2 * h :].T,
    )


def solution(mesh):
    rows, w_in, w_out = P("fs", None), P("fs", "tp"), P("tp", "fs")
    weights = (w_in, w_in, w_out) * 2

    return jax.shard_map(
        per_device,
        mesh=mesh,
        in_specs=(rows,) * 4 + (P(), P()) + weights + weights,
        out_specs=(rows,) * 3 + weights,
        check_vma=False,
    )
```

```python
import jax
import jax.numpy as jnp
from jax import lax
from jax.experimental import pallas as pl
from jax.experimental.pallas import tpu as pltpu
from jax.sharding import PartitionSpec as P

norm_eps = 1e-06
f32, bf16 = jnp.float32, jnp.bfloat16


def dot_nn(a, b):
    return jnp.dot(a, b, preferred_element_type=f32)


def dot_nt(a, b):
    return lax.dot_general(a, b, (((1,), (1,)), ((), ())), preferred_element_type=f32)


def dot_tn(a, b):
    return lax.dot_general(a, b, (((0,), (0,)), ((), ())), preferred_element_type=f32)


def row_factor(widened):
    return lax.rsqrt(jnp.mean(widened * widened, axis=-1, keepdims=True) + norm_eps)


def normalize(values, gain):
    widened = values.astype(f32)
    return (widened * row_factor(widened) * gain).astype(bf16)


def widen_cols(a, width):
    return jnp.concatenate([a, jnp.zeros((a.shape[0], width - a.shape[1]), a.dtype)], axis=1)


def forward_part(normed, w_in, w_down, h):
    pre = dot_nn(normed, w_in)
    gate, up = pre[:, :h], pre[:, h : 2 * h]
    hidden = (gate * jax.nn.sigmoid(gate) * up).astype(bf16)
    return dot_nt(widen_cols(hidden, w_down.shape[1]), w_down)


def backward_part(pre, cot, w_in, w_down, h):
    gate, up = pre[:, :h], pre[:, h : 2 * h]
    s = jax.nn.sigmoid(gate)
    activated = gate * s
    hidden = (activated * up).astype(bf16)
    hidden_grad = 0.5 * dot_nn(cot, w_down)[:, :h]
    gate_grad = hidden_grad * up * s * (1.0 + gate * (1.0 - s))
    both = jnp.concatenate([gate_grad, hidden_grad * activated], axis=1).astype(bf16)
    return dot_nt(widen_cols(both, w_in.shape[1]), w_in), both, hidden


def put_rows(send, part, at):
    rows = part.shape[0] // send.shape[0]
    for t in range(send.shape[0]):
        send[t, at : at + rows, :] = part[t * rows : (t + 1) * rows].astype(bf16)


def get_rows(whole, got, at):
    rows = whole.shape[0] // got.shape[0]
    for t in range(got.shape[0]):
        whole[t * rows : (t + 1) * rows, :] = got[t, at : at + rows, :]


def padded(n):
    return -(-n // 128) * 128


def sum_rows(got, at, rows):
    total = got[0, at : at + rows, :].astype(f32)
    for t in range(1, got.shape[0]):
        total = total + got[t, at : at + rows, :].astype(f32)
    return total


def forward_rows(late, branch):
    return (late.astype(f32) + 0.5 * branch).astype(bf16)


def backward_rows(early, cot, gain, normed_grad):
    widened = early.astype(f32)
    factor = row_factor(widened)
    scaled = normed_grad * gain
    unit = widened * factor
    mean = jnp.mean(scaled * unit, axis=-1, keepdims=True)
    return (cot.astype(f32) + factor * (scaled - unit * mean)).astype(bf16)


def weights_of(w, h, block):
    split = padded(2 * h)
    start = block * (split + padded(h))
    return w[:, start : start + split], w[:, start + split : start + split + padded(h)]


def backward_second(h, early, cot, gain, w, send, normed, both, hidden):
    w_in, w_down = weights_of(w, h, 1)
    rows = normalize(early[...], gain[...])
    normed[...] = rows
    part, both[...], hidden[...] = backward_part(dot_nn(rows, w_in), cot[...], w_in, w_down, h)
    put_rows(send, part, 0)


def forward_first(h, late, gain, w, send):
    w_in, w_down = weights_of(w, h, 0)
    put_rows(send, forward_part(normalize(late[...], gain[...]), w_in, w_down, h), 0)


def rows_b(got, early, cot, gain, other, send, own):
    rows = own.shape[0]
    own[...] = backward_rows(early[...], cot[...], gain[...], sum_rows(got, 0, rows))
    for t in range(send.shape[0]):
        send[t, :rows, :] = own[...]
        send[t, rows:, :] = other[t]


def backward_first(h, got, early, late, gain, w, send, normed, both, hidden, cot, own):
    rows = own.shape[0]
    w_in, w_down = weights_of(w, h, 0)
    get_rows(cot, got, 0)
    saved = normalize(early[...], gain[...])
    normed[...] = saved
    part, both[...], hidden[...] = backward_part(dot_nn(saved, w_in), cot[...], w_in, w_down, h)
    put_rows(send, part, rows)
    own[...] = forward_rows(late[...], sum_rows(got, rows, rows))
    for t in range(send.shape[0]):
        send[t, :rows, :] = own[...]


def middle(h, got, early, cot, gain_1, gain_2, w, send, late):
    rows = early.shape[0]
    get_rows(late, got, 0)
    w_in, w_down = weights_of(w, h, 1)
    part = forward_part(normalize(late[...], gain_2[...]), w_in, w_down, h)
    put_rows(send, part, 0)
    grad = backward_rows(early[...], cot[...], gain_1[...], sum_rows(got, rows, rows))
    for t in range(send.shape[0]):
        send[t, rows:, :] = grad


def last_rows(got, late, send, grad):
    rows = late.shape[0]
    out = forward_rows(late[...], sum_rows(got, 0, rows))
    get_rows(grad, got, rows)
    for t in range(send.shape[0]):
        send[t] = out


def near_parts(place, mine, got, own, right, left, top, bottom):
    half = top.shape[1]
    for k in range(own.shape[0]):
        for step in range(4):
            at = 4 * k + lax.rem(place[0] + step, 4)
            pair = (mine[at].astype(f32) + got[at].astype(f32)).astype(bf16)
            if step == 2:
                top[k] = pair[:half]
                bottom[k] = pair[half:]
            else:
                {0: own, 1: right, 3: left}[step][k] = pair


def far_parts(place, *refs):
    outs, scratch = refs[10:14], refs[14]
    for block in range(2):
        own, top, bottom, right, left = refs[5 * block : 5 * block + 5]
        half = top.shape[1]
        for k in range(own.shape[0]):
            total = own[k].astype(f32) + right[k].astype(f32) + left[k].astype(f32)
            scratch[k, :half] = (total[:half] + top[k].astype(f32)).astype(bf16)
            scratch[k, half:] = (total[half:] + bottom[k].astype(f32)).astype(bf16)
        for step in range(4):
            outs[step][block] = scratch[lax.rem(place[0] + step, 4)]


def block_products(normed, both, hidden, cot, z, size):
    cols = slice(z * size, (z + 1) * size)
    return dot_tn(normed[:, cols], both[...]), 0.5 * dot_tn(cot[:, cols], hidden[...])


def weight_parts_by_core(core, normed, both, hidden, cot, mine, theirs):
    rows, wide = mine.shape[1], both.shape[1]
    first = core[0] == 0
    for z in range(mine.shape[0]):
        for part, cols in zip(
            block_products(normed, both, hidden, cot, z, 2 * rows),
            (slice(0, wide), slice(wide, mine.shape[2])),
        ):
            top, bottom = part[:rows], part[rows:]
            mine[z, :, cols] = jnp.where(first, top, bottom).astype(bf16)
            theirs[z, :, cols] = jnp.where(first, bottom, top).astype(bf16)


def call(body, outs, *args, scalars=0, scratch=()):
    spaces = [pl.BlockSpec(memory_space=pltpu.SMEM)] * scalars
    spaces += [pl.BlockSpec(memory_space=pltpu.VMEM)] * (len(args) - scalars)
    return pl.pallas_call(
        body,
        in_specs=spaces,
        out_specs=[pl.BlockSpec(memory_space=pltpu.VMEM)] * len(outs),
        out_shape=[jax.ShapeDtypeStruct(shape, bf16) for shape in outs],
        scratch_shapes=[pltpu.VMEM(shape, bf16) for shape in scratch],
        compiler_params=pltpu.CompilerParams(vmem_limit_bytes=48 * 2**20),
    )(*args)


def own_rows(a):
    rows = a.shape[0] // lax.axis_size("tp")
    return lax.dynamic_slice_in_dim(a, lax.axis_index("tp") * rows, rows, axis=0)


def exchange(a):
    return lax.all_to_all(a, "tp", split_axis=0, concat_axis=0, tiled=True)


def moved(a, step):
    n = lax.axis_size("fs")
    return lax.ppermute(a, "fs", [(q, (q + 2 * step) % n) for q in range(n)])


def swapped(a):
    n = lax.axis_size("fs")
    return lax.ppermute(a, "fs", [(q, q ^ 1) for q in range(n)])


def near_level(core, z, saved, cot, n_fs, d, h):
    block = (n_fs // 2, d // n_fs, 3 * h)
    mine, theirs = call(weight_parts_by_core, (block, block), core, *saved, cot, scalars=1)
    quarter = (4,) + block[1:]
    half = (4, block[1] // 2, block[2])
    got = swapped(theirs)
    own, right, left, top, bottom = call(
        near_parts, (quarter,) * 3 + (half,) * 2, z, mine, got, scalars=1
    )
    return own, moved(top, -2), moved(bottom, 2), moved(right, 1), moved(left, -1)


def far_level(kz, *parts):
    block = parts[0].shape
    outs = call(
        far_parts, ((2,) + block[1:],) * 4, kz, *parts, scalars=1, scratch=(block,)
    )
    across = moved(outs[2], 8)
    up, down = moved(outs[1], 4), moved(outs[3], -4)
    return outs[0].astype(f32) + up.astype(f32) + down.astype(f32) + across.astype(f32)


def pack(gate, up, down):
    h = gate.shape[1]
    return jnp.concatenate(
        [
            gate,
            jnp.pad(up, ((0, 0), (0, padded(2 * h) - 2 * h))),
            jnp.pad(down.T, ((0, 0), (0, padded(h) - h))),
        ],
        axis=1,
    )


def per_device(
    late_input,
    early_input,
    early_mid,
    cotangent,
    gain_first,
    gain_second,
    gate_first,
    up_first,
    down_first,
    gate_second,
    up_second,
    down_second,
    sum_gate_first,
    sum_up_first,
    sum_down_first,
    sum_gate_second,
    sum_up_second,
    sum_down_second,
):
    h = gate_first.shape[1]
    tokens, d = late_input.shape
    n = lax.axis_size("tp")
    n_fs = lax.axis_size("fs")
    rows = tokens // n
    gain_1, gain_2 = gain_first[None], gain_second[None]
    index = lax.axis_index("fs").astype(jnp.int32)
    core, z, kz = ((i.astype(jnp.int32))[None] for i in (index % 2, index // 2 % 4, index // 8))
    late_own, early_own, mid_own, cot_own = (
        own_rows(a) for a in (late_input, early_input, early_mid, cotangent)
    )
    packed = jnp.concatenate(
        [pack(gate_first, up_first, down_first), pack(gate_second, up_second, down_second)], axis=1
    )
    w = lax.all_gather(packed, "fs", axis=0, tiled=True)

    single, double = (n, rows, d), (n, 2 * rows, d)
    saved_shapes = ((tokens, d), (tokens, 2 * h), (tokens, h))
    send, *saved_second = call(
        lambda *refs: backward_second(h, *refs), (single,) + saved_shapes,
        early_mid, cotangent, gain_2, w,
    )
    got = exchange(send)
    (send_f,) = call(
        lambda *refs: forward_first(h, *refs), (single,), late_input, gain_1, w
    )
    send, mid_rows = call(rows_b, (double, (rows, d)), got, mid_own, cot_own, gain_2, send_f)
    got = exchange(send)
    near_2 = near_level(core, z, saved_second, cotangent, n_fs, d, h)

    send, *saved_first, mid_grad, late_rows = call(
        lambda *refs: backward_first(h, *refs),
        (double,) + saved_shapes + ((tokens, d), (rows, d)),
        got, early_input, late_own, gain_1, w,
    )
    got = exchange(send)
    near_1 = near_level(core, z, saved_first, mid_grad, n_fs, d, h)

    send, late_mid = call(
        lambda *refs: middle(h, *refs), (double, (tokens, d)),
        got, early_own, mid_rows, gain_1, gain_2, w,
    )
    got = exchange(send)
    g2, g1 = far_level(kz, *near_2, *near_1)
    send, input_grad = call(last_rows, (single, (tokens, d)), got, late_rows)
    late_out = exchange(send).reshape(tokens, d)
    return (
        late_mid,
        late_out,
        input_grad,
        sum_gate_first + g1[:, :h],
        sum_up_first + g1[:, h : 2 * h],
        sum_down_first + g1[:, 2 * h :].T,
        sum_gate_second + g2[:, :h],
        sum_up_second + g2[:, h : 2 * h],
        sum_down_second + g2[:, 2 * h :].T,
    )


def solution(mesh):
    rows, w_in, w_out = P("fs", None), P("fs", "tp"), P("tp", "fs")
    weights = (w_in, w_in, w_out) * 2

    return jax.shard_map(
        per_device,
        mesh=mesh,
        in_specs=(rows,) * 4 + (P(), P()) + weights + weights,
        out_specs=(rows,) * 3 + weights,
        check_vma=False,
    )
```

```python
import jax
import jax.numpy as jnp
from jax import lax
from jax.experimental import pallas as pl
from jax.experimental.pallas import tpu as pltpu
from jax.sharding import PartitionSpec as P

norm_eps = 1e-06
f32, bf16 = jnp.float32, jnp.bfloat16


def dot_nn(a, b):
    return jnp.dot(a, b, preferred_element_type=f32)


def dot_nt(a, b):
    return lax.dot_general(a, b, (((1,), (1,)), ((), ())), preferred_element_type=f32)


def dot_tn(a, b):
    return lax.dot_general(a, b, (((0,), (0,)), ((), ())), preferred_element_type=f32)


def row_factor(widened):
    return lax.rsqrt(jnp.mean(widened * widened, axis=-1, keepdims=True) + norm_eps)


def normalize(values, gain):
    widened = values.astype(f32)
    return (widened * row_factor(widened) * gain).astype(bf16)


def widen_cols(a, width):
    return jnp.concatenate([a, jnp.zeros((a.shape[0], width - a.shape[1]), a.dtype)], axis=1)


def forward_part(normed, w_in, w_down, h):
    pre = dot_nn(normed, w_in)
    gate, up = pre[:, :h], pre[:, h : 2 * h]
    hidden = (gate * jax.nn.sigmoid(gate) * up).astype(bf16)
    return dot_nt(widen_cols(hidden, w_down.shape[1]), w_down)


def backward_part(pre, cot, w_in, w_down, h):
    gate, up = pre[:, :h], pre[:, h : 2 * h]
    s = jax.nn.sigmoid(gate)
    activated = gate * s
    hidden = (activated * up).astype(bf16)
    hidden_grad = 0.5 * dot_nn(cot, w_down)[:, :h]
    gate_grad = hidden_grad * up * s * (1.0 + gate * (1.0 - s))
    both = jnp.concatenate([gate_grad, hidden_grad * activated], axis=1).astype(bf16)
    return dot_nt(widen_cols(both, w_in.shape[1]), w_in), both, hidden


def put_rows(send, part, at):
    rows = part.shape[0] // send.shape[0]
    for t in range(send.shape[0]):
        send[t, at : at + rows, :] = part[t * rows : (t + 1) * rows].astype(bf16)


def get_rows(whole, got, at):
    rows = whole.shape[0] // got.shape[0]
    for t in range(got.shape[0]):
        whole[t * rows : (t + 1) * rows, :] = got[t, at : at + rows, :]


def padded(n):
    return -(-n // 128) * 128


def sum_rows(got, at, rows):
    total = got[0, at : at + rows, :].astype(f32)
    for t in range(1, got.shape[0]):
        total = total + got[t, at : at + rows, :].astype(f32)
    return total


def forward_rows(late, branch):
    return (late.astype(f32) + 0.5 * branch).astype(bf16)


def backward_rows(early, cot, gain, normed_grad):
    widened = early.astype(f32)
    factor = row_factor(widened)
    scaled = normed_grad * gain
    unit = widened * factor
    mean = jnp.mean(scaled * unit, axis=-1, keepdims=True)
    return (cot.astype(f32) + factor * (scaled - unit * mean)).astype(bf16)


def start_copies(pairs, sems):
    copies = [pltpu.make_async_copy(a, b, sems.at[k]) for k, (a, b) in enumerate(pairs)]
    for copy in copies:
        copy.start()
    return copies


def weights_of(w, h, block):
    split = padded(2 * h)
    start = block * (split + padded(h))
    return w.at[:, start : start + split], w.at[:, start + split : start + split + padded(h)]


def backward_second(h, early, cot, gain, w, send, normed, both, hidden, v_in, v_down, v_early, v_cot, sems):
    w_in, w_down = weights_of(w, h, 1)
    copies = start_copies(
        ((early, v_early), (w_in, v_in), (cot, v_cot), (w_down, v_down)), sems
    )
    copies[0].wait()
    rows = normalize(v_early[...], gain[...])
    normed[...] = rows
    copies[1].wait()
    pre = dot_nn(rows, v_in[...])
    copies[2].wait()
    copies[3].wait()
    part, both[...], hidden[...] = backward_part(pre, v_cot[...], v_in[...], v_down[...], h)
    put_rows(send, part, 0)


def forward_first(h, late, gain, w, send, v_in, v_down, v_late, sems):
    w_in, w_down = weights_of(w, h, 0)
    copies = start_copies(((late, v_late), (w_in, v_in), (w_down, v_down)), sems)
    for copy in copies:
        copy.wait()
    put_rows(send, forward_part(normalize(v_late[...], gain[...]), v_in[...], v_down[...], h), 0)


def rows_b(got, early, cot, gain, other, send, own):
    rows = own.shape[0]
    own[...] = backward_rows(early[...], cot[...], gain[...], sum_rows(got, 0, rows))
    for t in range(send.shape[0]):
        send[t, :rows, :] = own[...]
        send[t, rows:, :] = other[t]


def backward_first(
    h, got, early, late, gain, w, send, normed, both, hidden, cot, own, v_in, v_down, v_early, sems
):
    rows = own.shape[0]
    w_in, w_down = weights_of(w, h, 0)
    copies = start_copies(((early, v_early), (w_in, v_in), (w_down, v_down)), sems)
    get_rows(cot, got, 0)
    own[...] = forward_rows(late[...], sum_rows(got, rows, rows))
    for t in range(send.shape[0]):
        send[t, :rows, :] = own[...]
    copies[0].wait()
    saved = normalize(v_early[...], gain[...])
    normed[...] = saved
    copies[1].wait()
    pre = dot_nn(saved, v_in[...])
    copies[2].wait()
    part, both[...], hidden[...] = backward_part(pre, cot[...], v_in[...], v_down[...], h)
    put_rows(send, part, rows)


def middle(h, got, early, cot, gain_1, gain_2, w, send, late, v_in, v_down, sems):
    rows = early.shape[0]
    w_in, w_down = weights_of(w, h, 1)
    copies = start_copies(((w_in, v_in), (w_down, v_down)), sems)
    get_rows(late, got, 0)
    grad = backward_rows(early[...], cot[...], gain_1[...], sum_rows(got, rows, rows))
    for t in range(send.shape[0]):
        send[t, rows:, :] = grad
    normed = normalize(late[...], gain_2[...])
    for copy in copies:
        copy.wait()
    put_rows(send, forward_part(normed, v_in[...], v_down[...], h), 0)


def last_rows(got, late, send, grad):
    rows = late.shape[0]
    out = forward_rows(late[...], sum_rows(got, 0, rows))
    get_rows(grad, got, rows)
    for t in range(send.shape[0]):
        send[t] = out


def near_parts(place, mine, got, own, right, left, top, bottom):
    half = top.shape[1]
    for k in range(own.shape[0]):
        for step in range(4):
            at = 4 * k + lax.rem(place[0] + step, 4)
            pair = (mine[at].astype(f32) + got[at].astype(f32)).astype(bf16)
            if step == 2:
                top[k] = pair[:half]
                bottom[k] = pair[half:]
            else:
                {0: own, 1: right, 3: left}[step][k] = pair


def pair_sum(mine, got, out):
    for z in range(out.shape[0]):
        out[z] = (mine[z].astype(f32) + got[z].astype(f32)).astype(bf16)


def far_parts(place, own, top, bottom, right, left, here, up, across, down, scratch):
    half = top.shape[1]
    for k in range(own.shape[0]):
        total = own[k].astype(f32) + right[k].astype(f32) + left[k].astype(f32)
        scratch[k, :half] = (total[:half] + top[k].astype(f32)).astype(bf16)
        scratch[k, half:] = (total[half:] + bottom[k].astype(f32)).astype(bf16)
    for step, out in enumerate((here, up, across, down)):
        out[...] = scratch[lax.rem(place[0] + step, 4)]


def pack_weights(*refs):
    out = refs[6]
    rows, h = refs[0].shape
    pad_in, pad_down = padded(2 * h) - 2 * h, padded(h) - h
    parts = []
    for gate, up, down in (refs[:3], refs[3:6]):
        zeros = jnp.zeros((rows, pad_in + pad_down), bf16)
        parts += [gate[...], up[...], zeros[:, :pad_in], down[...], zeros[:, :pad_down]]
    out[...] = jnp.concatenate(parts, axis=1)


def block_products(normed, both, hidden, cot, z, size):
    cols = slice(z * size, (z + 1) * size)
    return dot_tn(normed[:, cols], both[...]), 0.5 * dot_tn(cot[:, cols], hidden[...])


def weight_parts_by_core(core, normed, both, hidden, cot, mine, theirs):
    rows, wide = mine.shape[1], both.shape[1]
    first = core[0] == 0
    for z in range(mine.shape[0]):
        for part, cols in zip(
            block_products(normed, both, hidden, cot, z, 2 * rows),
            (slice(0, wide), slice(wide, mine.shape[2])),
        ):
            top, bottom = part[:rows], part[rows:]
            mine[z, :, cols] = jnp.where(first, top, bottom).astype(bf16)
            theirs[z, :, cols] = jnp.where(first, bottom, top).astype(bf16)


def call(body, outs, *args, scalars=0, scratch=(), copied=()):
    spaces = [
        pltpu.SMEM if k < scalars else pl.ANY if k in copied else pltpu.VMEM
        for k in range(len(args))
    ]
    sems = [pltpu.SemaphoreType.DMA((len(scratch),))] if copied else []
    return pl.pallas_call(
        body,
        in_specs=[pl.BlockSpec(memory_space=space) for space in spaces],
        out_specs=[pl.BlockSpec(memory_space=pltpu.VMEM)] * len(outs),
        out_shape=[jax.ShapeDtypeStruct(shape, bf16) for shape in outs],
        scratch_shapes=[pltpu.VMEM(shape, bf16) for shape in scratch] + sems,
        compiler_params=pltpu.CompilerParams(vmem_limit_bytes=48 * 2**20),
    )(*args)


def own_rows(a):
    rows = a.shape[0] // lax.axis_size("tp")
    return lax.dynamic_slice_in_dim(a, lax.axis_index("tp") * rows, rows, axis=0)


def exchange(a):
    return lax.all_to_all(a, "tp", split_axis=0, concat_axis=0, tiled=True)


def moved(a, step):
    n = lax.axis_size("fs")
    return lax.ppermute(a, "fs", [(q, (q + 2 * step) % n) for q in range(n)])


def swapped(a):
    n = lax.axis_size("fs")
    return lax.ppermute(a, "fs", [(q, q ^ 1) for q in range(n)])


def swapped_parts(core, saved, cot, n_fs, d, h):
    block = (n_fs // 2, d // n_fs, 3 * h)
    mine, theirs = call(weight_parts_by_core, (block, block), core, *saved, cot, scalars=1)
    return mine, swapped(theirs)


def reduce_offloaded(mine, got):
    n = lax.axis_size("fs")
    groups = [[2 * z + c for z in range(n // 2)] for c in range(2)]
    (pair,) = call(pair_sum, (mine.shape,), mine, got)
    return lax.psum_scatter(
        pair.reshape(-1, pair.shape[2]), "fs",
        scatter_dimension=0, tiled=True, axis_index_groups=groups,
    )


def near_level(z, mine, got):
    block = mine.shape
    quarter = (4,) + block[1:]
    half = (4, block[1] // 2, block[2])
    own, right, left, top, bottom = call(
        near_parts, (quarter,) * 3 + (half,) * 2, z, mine, got, scalars=1
    )
    return own, moved(top, -2), moved(bottom, 2), moved(right, 1), moved(left, -1)


def far_level(kz, *parts):
    block = parts[0].shape
    here, up, across, down = call(
        far_parts, (block[1:],) * 4, kz, *parts, scalars=1, scratch=(block,)
    )
    across = moved(across, 8)
    up, down = moved(up, 4), moved(down, -4)
    return here.astype(f32) + up.astype(f32) + down.astype(f32) + across.astype(f32)


def per_device(
    late_input,
    early_input,
    early_mid,
    cotangent,
    gain_first,
    gain_second,
    gate_first,
    up_first,
    down_first,
    gate_second,
    up_second,
    down_second,
    sum_gate_first,
    sum_up_first,
    sum_down_first,
    sum_gate_second,
    sum_up_second,
    sum_down_second,
):
    h = gate_first.shape[1]
    tokens, d = late_input.shape
    n = lax.axis_size("tp")
    n_fs = lax.axis_size("fs")
    rows = tokens // n
    gain_1, gain_2 = gain_first[None], gain_second[None]
    index = lax.axis_index("fs").astype(jnp.int32)
    core, z, kz = ((i.astype(jnp.int32))[None] for i in (index % 2, index // 2 % 4, index // 8))
    late_own, early_own, mid_own, cot_own = (
        own_rows(a) for a in (late_input, early_input, early_mid, cotangent)
    )
    wide = 2 * (padded(2 * h) + padded(h))
    (packed,) = call(
        pack_weights, ((gate_first.shape[0], wide),),
        gate_first, up_first, down_first.T, gate_second, up_second, down_second.T,
    )
    w = lax.all_gather(packed, "fs", axis=0, tiled=True)

    single, double = (n, rows, d), (n, 2 * rows, d)
    saved_shapes = ((tokens, d), (tokens, 2 * h), (tokens, h))
    held = ((d, padded(2 * h)), (d, padded(h)))
    whole = (tokens, d)
    send, *saved_second = call(
        lambda *refs: backward_second(h, *refs), (single,) + saved_shapes,
        early_mid, cotangent, gain_2, w, copied=(0, 1, 3), scratch=held + (whole, whole),
    )
    got = exchange(send)
    pieces_2 = swapped_parts(core, saved_second, cotangent, n_fs, d, h)
    (send_f,) = call(
        lambda *refs: forward_first(h, *refs), (single,), late_input, gain_1, w,
        copied=(0, 2), scratch=held + (whole,),
    )
    send, mid_rows = call(rows_b, (double, (rows, d)), got, mid_own, cot_own, gain_2, send_f)
    got = exchange(send)
    g2 = reduce_offloaded(*pieces_2)

    send, *saved_first, mid_grad, late_rows = call(
        lambda *refs: backward_first(h, *refs), (double,) + saved_shapes + (whole, (rows, d)),
        got, early_input, late_own, gain_1, w, copied=(1, 4), scratch=held + (whole,),
    )
    got = exchange(send)
    near = near_level(z, *swapped_parts(core, saved_first, mid_grad, n_fs, d, h))

    send, late_mid = call(
        lambda *refs: middle(h, *refs), (double, whole),
        got, early_own, mid_rows, gain_1, gain_2, w, copied=(5,), scratch=held,
    )
    got = exchange(send)
    g1 = far_level(kz, *near)
    send, input_grad = call(last_rows, (single, whole), got, late_rows)
    late_out = exchange(send).reshape(tokens, d)
    g1, g2 = lax.optimization_barrier((g1, g2))
    g2 = g2.astype(f32)
    return (
        late_mid,
        late_out,
        input_grad,
        sum_gate_first + g1[:, :h],
        sum_up_first + g1[:, h : 2 * h],
        sum_down_first + g1[:, 2 * h :].T,
        sum_gate_second + g2[:, :h],
        sum_up_second + g2[:, h : 2 * h],
        sum_down_second + g2[:, 2 * h :].T,
    )


def solution(mesh):
    rows, w_in, w_out = P("fs", None), P("fs", "tp"), P("tp", "fs")
    weights = (w_in, w_in, w_out) * 2

    return jax.shard_map(
        per_device,
        mesh=mesh,
        in_specs=(rows,) * 4 + (P(), P()) + weights + weights,
        out_specs=(rows,) * 3 + weights,
        check_vma=False,
    )
```

```python
import jax
import jax.numpy as jnp
from jax import lax
from jax.experimental import pallas as pl
from jax.experimental.pallas import tpu as pltpu
from jax.sharding import PartitionSpec as P

norm_eps = 1e-06
f32, bf16 = jnp.float32, jnp.bfloat16


def dot_nn(a, b):
    return jnp.dot(a, b, preferred_element_type=f32)


def dot_nt(a, b):
    return lax.dot_general(a, b, (((1,), (1,)), ((), ())), preferred_element_type=f32)


def dot_tn(a, b):
    return lax.dot_general(a, b, (((0,), (0,)), ((), ())), preferred_element_type=f32)


def row_factor(widened):
    return lax.rsqrt(jnp.mean(widened * widened, axis=-1, keepdims=True) + norm_eps)


def normalize(values, gain):
    widened = values.astype(f32)
    return (widened * row_factor(widened) * gain).astype(bf16)


def widen_cols(a, width):
    return jnp.concatenate([a, jnp.zeros((a.shape[0], width - a.shape[1]), a.dtype)], axis=1)


def forward_part(normed, w_in, w_down, h):
    pre = dot_nn(normed, w_in)
    gate, up = pre[:, :h], pre[:, h : 2 * h]
    hidden = (gate * jax.nn.sigmoid(gate) * up).astype(bf16)
    return dot_nt(widen_cols(hidden, w_down.shape[1]), w_down)


def backward_part(pre, cot, w_in, w_down, h):
    gate, up = pre[:, :h], pre[:, h : 2 * h]
    s = jax.nn.sigmoid(gate)
    activated = gate * s
    hidden = (activated * up).astype(bf16)
    hidden_grad = 0.5 * dot_nn(cot, w_down)[:, :h]
    gate_grad = hidden_grad * up * s * (1.0 + gate * (1.0 - s))
    both = jnp.concatenate([gate_grad, hidden_grad * activated], axis=1).astype(bf16)
    return dot_nt(widen_cols(both, w_in.shape[1]), w_in), both, hidden


def put_rows(send, part, at):
    rows = part.shape[0] // send.shape[0]
    for t in range(send.shape[0]):
        send[t, at : at + rows, :] = part[t * rows : (t + 1) * rows].astype(bf16)


def get_rows(whole, got, at):
    rows = whole.shape[0] // got.shape[0]
    for t in range(got.shape[0]):
        whole[t * rows : (t + 1) * rows, :] = got[t, at : at + rows, :]


def padded(n):
    return -(-n // 128) * 128


def sum_rows(got, at, rows):
    total = got[0, at : at + rows, :].astype(f32)
    for t in range(1, got.shape[0]):
        total = total + got[t, at : at + rows, :].astype(f32)
    return total


def forward_rows(late, branch):
    return (late.astype(f32) + 0.5 * branch).astype(bf16)


def backward_rows(early, cot, gain, normed_grad):
    widened = early.astype(f32)
    factor = row_factor(widened)
    scaled = normed_grad * gain
    unit = widened * factor
    mean = jnp.mean(scaled * unit, axis=-1, keepdims=True)
    return (cot.astype(f32) + factor * (scaled - unit * mean)).astype(bf16)


def start_copies(pairs, sems):
    copies = [pltpu.make_async_copy(a, b, sems.at[k]) for k, (a, b) in enumerate(pairs)]
    for copy in copies:
        copy.start()
    return copies


def weights_of(w, h, block):
    split = padded(2 * h)
    start = block * (split + padded(h))
    return w.at[:, start : start + split], w.at[:, start + split : start + split + padded(h)]


def stage_one(
    h, late, early, cot, gain_1, gain_2, w, send, normed, both, hidden,
    v_in, v_down, v_in_1, v_down_1, v_early, v_cot, v_late, sems,
):
    w_in, w_down = weights_of(w, h, 1)
    w_in_1, w_down_1 = weights_of(w, h, 0)
    copies = start_copies(
        (
            (early, v_early), (w_in, v_in), (cot, v_cot), (w_down, v_down),
            (late, v_late), (w_in_1, v_in_1), (w_down_1, v_down_1),
        ),
        sems,
    )
    copies[0].wait()
    saved = normalize(v_early[...], gain_2[...])
    normed[...] = saved
    copies[1].wait()
    pre = dot_nn(saved, v_in[...])
    copies[2].wait()
    copies[3].wait()
    part, both[...], hidden[...] = backward_part(pre, v_cot[...], v_in[...], v_down[...], h)
    put_rows(send, part, send.shape[1] // 2)
    for copy in copies[4:]:
        copy.wait()
    rows = normalize(v_late[...], gain_1[...])
    put_rows(send, forward_part(rows, v_in_1[...], v_down_1[...], h), 0)


def recompute(h, early, gain, w, normed, pre, v_in, v_early, sems):
    copies = start_copies(((early, v_early), (weights_of(w, h, 0)[0], v_in)), sems)
    copies[0].wait()
    rows = normalize(v_early[...], gain[...])
    normed[...] = rows
    copies[1].wait()
    pre[...] = dot_nn(rows, v_in[...])


def stage_two(
    h, got, pre, gain_2, w, late, cot, send, both, hidden, v_in, v_down, v_in_2, v_down_2, sems
):
    w_in, w_down = weights_of(w, h, 0)
    w_in_2, w_down_2 = weights_of(w, h, 1)
    copies = start_copies(
        ((w_down, v_down), (w_in, v_in), (w_in_2, v_in_2), (w_down_2, v_down_2)), sems
    )
    rows = got.shape[1] // 2
    get_rows(cot, got, rows)
    get_rows(late, got, 0)
    copies[0].wait()
    copies[1].wait()
    part, both[...], hidden[...] = backward_part(pre[...], cot[...], v_in[...], v_down[...], h)
    put_rows(send, part, rows)
    normed = normalize(late[...], gain_2[...])
    copies[2].wait()
    copies[3].wait()
    put_rows(send, forward_part(normed, v_in_2[...], v_down_2[...], h), 0)


def update_rows(got, late, early, cot, gain, send, own):
    rows = late.shape[0]
    own[:rows, :] = forward_rows(late[...], sum_rows(got, 0, rows))
    own[rows:, :] = backward_rows(early[...], cot[...], gain[...], sum_rows(got, rows, rows))
    for t in range(send.shape[0]):
        send[t] = own[...]


def pair_sum(mine, got, out):
    for z in range(out.shape[0]):
        out[z] = (mine[z].astype(f32) + got[z].astype(f32)).astype(bf16)


def near_parts(place, mine, got, *outs):
    for k in range(outs[0].shape[0]):
        for step, out in enumerate(outs):
            at = 4 * k + place[step]
            out[k] = (mine[at].astype(f32) + got[at].astype(f32)).astype(bf16)


def far_parts(place, own, one, back, two, here, up, across, down, scratch):
    for k in range(own.shape[0]):
        scratch[k] = (
            own[k].astype(f32) + one[k].astype(f32) + back[k].astype(f32) + two[k].astype(f32)
        ).astype(bf16)
    for step, out in enumerate((here, up, across, down)):
        out[...] = scratch[lax.rem(place[0] + step, 4)]


def pack_weights(*refs):
    out = refs[6]
    rows, h = refs[0].shape
    pad_in, pad_down = padded(2 * h) - 2 * h, padded(h) - h
    parts = []
    for gate, up, down in (refs[:3], refs[3:6]):
        zeros = jnp.zeros((rows, pad_in + pad_down), bf16)
        parts += [gate[...], up[...], zeros[:, :pad_in], down[...], zeros[:, :pad_down]]
    out[...] = jnp.concatenate(parts, axis=1)


def block_products(normed, both, hidden, cot, z, size):
    cols = slice(z * size, (z + 1) * size)
    return dot_tn(normed[:, cols], both[...]), 0.5 * dot_tn(cot[:, cols], hidden[...])


def weight_parts_by_core(core, normed, both, hidden, cot, mine, theirs):
    rows, wide = mine.shape[1], both.shape[1]
    first = core[0] == 0
    for z in range(mine.shape[0]):
        for part, cols in zip(
            block_products(normed, both, hidden, cot, z, 2 * rows),
            (slice(0, wide), slice(wide, mine.shape[2])),
        ):
            top, bottom = part[:rows], part[rows:]
            mine[z, :, cols] = jnp.where(first, top, bottom).astype(bf16)
            theirs[z, :, cols] = jnp.where(first, bottom, top).astype(bf16)


def call(body, outs, *args, scalars=0, scratch=(), copied=()):
    spaces = [
        pltpu.SMEM if k < scalars else pl.ANY if k in copied else pltpu.VMEM
        for k in range(len(args))
    ]
    sems = [pltpu.SemaphoreType.DMA((len(scratch),))] if copied else []
    return pl.pallas_call(
        body,
        in_specs=[pl.BlockSpec(memory_space=space) for space in spaces],
        out_specs=[pl.BlockSpec(memory_space=pltpu.VMEM)] * len(outs),
        out_shape=[
            jax.ShapeDtypeStruct(shape[:-1], f32)
            if shape[-1] is f32
            else jax.ShapeDtypeStruct(shape, bf16)
            for shape in outs
        ],
        scratch_shapes=[pltpu.VMEM(shape, bf16) for shape in scratch] + sems,
        compiler_params=pltpu.CompilerParams(vmem_limit_bytes=48 * 2**20),
    )(*args)


def own_rows(a):
    rows = a.shape[0] // lax.axis_size("tp")
    return lax.dynamic_slice_in_dim(a, lax.axis_index("tp") * rows, rows, axis=0)


def exchange(a):
    return lax.all_to_all(a, "tp", split_axis=0, concat_axis=0, tiled=True)


def moved(a, step, mirror=False):
    n = lax.axis_size("fs")
    sign = [1, -1 if mirror else 1]
    return lax.ppermute(a, "fs", [(q, (q + 2 * step * sign[q % 2]) % n) for q in range(n)])


def swapped(a):
    n = lax.axis_size("fs")
    return lax.ppermute(a, "fs", [(q, q ^ 1) for q in range(n)])


def swapped_parts(core, saved, cot, n_fs, d, h):
    block = (n_fs // 2, d // n_fs, 3 * h)
    mine, theirs = call(weight_parts_by_core, (block, block), core, *saved, cot, scalars=1)
    return mine, swapped(theirs)


def reduce_offloaded(mine, got):
    n = lax.axis_size("fs")
    groups = [[2 * z + c for z in range(n // 2)] for c in range(2)]
    (pair,) = call(pair_sum, (mine.shape,), mine, got)
    return lax.psum_scatter(
        pair.reshape(-1, pair.shape[2]), "fs",
        scatter_dimension=0, tiled=True, axis_index_groups=groups,
    )


def near_level(core, z, mine, got):
    steps = (0, 1, -1, -2)
    classes = jnp.stack([(z + step * (1 - 2 * core)) % 4 for step in steps]).astype(jnp.int32)
    own, *parts = call(
        near_parts, ((4,) + mine.shape[1:],) * 4, classes, mine, got, scalars=1
    )
    return own, *(moved(part, step, mirror=True) for part, step in zip(parts, steps[1:]))


def far_level(kz, *parts):
    block = parts[0].shape
    here, up, across, down = call(
        far_parts, (block[1:],) * 4, kz, *parts, scalars=1, scratch=(block,)
    )
    across = moved(across, 8)
    up, down = moved(up, 4), moved(down, -4)
    return here.astype(f32) + up.astype(f32) + down.astype(f32) + across.astype(f32)


def per_device(
    late_input,
    early_input,
    early_mid,
    cotangent,
    gain_first,
    gain_second,
    gate_first,
    up_first,
    down_first,
    gate_second,
    up_second,
    down_second,
    sum_gate_first,
    sum_up_first,
    sum_down_first,
    sum_gate_second,
    sum_up_second,
    sum_down_second,
):
    h = gate_first.shape[1]
    tokens, d = late_input.shape
    n = lax.axis_size("tp")
    n_fs = lax.axis_size("fs")
    rows = tokens // n
    gain_1, gain_2 = gain_first[None], gain_second[None]
    index = lax.axis_index("fs").astype(jnp.int32)
    core, kz = (i.astype(jnp.int32)[None] for i in (index % 2, index // 8))
    late_own, early_own, mid_own, cot_own = (
        own_rows(a) for a in (late_input, early_input, early_mid, cotangent)
    )
    wide = 2 * (padded(2 * h) + padded(h))
    (packed,) = call(
        pack_weights, ((gate_first.shape[0], wide),),
        gate_first, up_first, down_first.T, gate_second, up_second, down_second.T,
    )
    w = lax.all_gather(packed, "fs", axis=0, tiled=True)

    double, whole = (n, 2 * rows, d), (tokens, d)
    saved_shapes = (whole, (tokens, 2 * h), (tokens, h))
    held = ((d, padded(2 * h)), (d, padded(h)))
    send, *saved_second = call(
        lambda *refs: stage_one(h, *refs), (double,) + saved_shapes,
        late_input, early_mid, cotangent, gain_1, gain_2, w,
        copied=(0, 1, 2, 5), scratch=held + held + (whole,) * 3,
    )
    got = exchange(send)
    pieces_2 = swapped_parts(core, saved_second, cotangent, n_fs, d, h)
    normed, pre = call(
        lambda *refs: recompute(h, *refs), (whole, (tokens, padded(2 * h), f32)),
        early_input, gain_1, w, copied=(0, 2), scratch=held[:1] + (whole,),
    )
    send, own = call(
        update_rows, (double, (2 * rows, d)), got, late_own, mid_own, cot_own, gain_2
    )
    got = exchange(send)
    g2 = reduce_offloaded(*pieces_2)

    late_mid, mid_grad, send, *saved_first = call(
        lambda *refs: stage_two(h, *refs), (whole, whole, double) + saved_shapes[1:],
        got, pre, gain_2, w, copied=(3,), scratch=held + held,
    )
    got = exchange(send)
    pieces_1 = swapped_parts(core, (normed, *saved_first), mid_grad, n_fs, d, h)
    near = near_level(core[0], index // 2, *pieces_1)
    send, _ = call(
        update_rows, (double, (2 * rows, d)), got, own[:rows], early_own, own[rows:], gain_1
    )
    got = exchange(send)
    g1 = far_level(kz, *near)
    late_out = got[:, :rows].reshape(whole)
    input_grad = got[:, rows:].reshape(whole)
    g1, g2 = lax.optimization_barrier((g1, g2))
    g2 = g2.astype(f32)
    return (
        late_mid,
        late_out,
        input_grad,
        sum_gate_first + g1[:, :h],
        sum_up_first + g1[:, h : 2 * h],
        sum_down_first + g1[:, 2 * h :].T,
        sum_gate_second + g2[:, :h],
        sum_up_second + g2[:, h : 2 * h],
        sum_down_second + g2[:, 2 * h :].T,
    )


def solution(mesh):
    rows, w_in, w_out = P("fs", None), P("fs", "tp"), P("tp", "fs")
    weights = (w_in, w_in, w_out) * 2

    return jax.shard_map(
        per_device,
        mesh=mesh,
        in_specs=(rows,) * 4 + (P(), P()) + weights + weights,
        out_specs=(rows,) * 3 + weights,
        check_vma=False,
    )
```

```python
import jax
import jax.numpy as jnp
from jax import lax
from jax.experimental import pallas as pl
from jax.experimental.pallas import tpu as pltpu
from jax.sharding import PartitionSpec as P

norm_eps = 1e-06
f32, bf16 = jnp.float32, jnp.bfloat16


def dot_nn(a, b):
    return jnp.dot(a, b, preferred_element_type=f32)


def dot_nt(a, b):
    return lax.dot_general(a, b, (((1,), (1,)), ((), ())), preferred_element_type=f32)


def dot_tn(a, b):
    return lax.dot_general(a, b, (((0,), (0,)), ((), ())), preferred_element_type=f32)


def row_factor(widened):
    return lax.rsqrt(jnp.mean(widened * widened, axis=-1, keepdims=True) + norm_eps)


def normalize(values, gain):
    widened = values.astype(f32)
    return (widened * row_factor(widened) * gain).astype(bf16)


def widen_cols(a, width):
    return jnp.concatenate([a, jnp.zeros((a.shape[0], width - a.shape[1]), a.dtype)], axis=1)


def forward_part(normed, w_in, w_down, h):
    pre = dot_nn(normed, w_in)
    gate, up = pre[:, :h], pre[:, h : 2 * h]
    hidden = (gate * jax.nn.sigmoid(gate) * up).astype(bf16)
    return dot_nt(widen_cols(hidden, w_down.shape[1]), w_down)


def backward_part(pre, cot, w_in, w_down, h):
    gate, up = pre[:, :h], pre[:, h : 2 * h]
    s = jax.nn.sigmoid(gate)
    activated = gate * s
    hidden = (activated * up).astype(bf16)
    hidden_grad = 0.5 * dot_nn(cot, w_down)[:, :h]
    gate_grad = hidden_grad * up * s * (1.0 + gate * (1.0 - s))
    both = jnp.concatenate([gate_grad, hidden_grad * activated], axis=1).astype(bf16)
    return dot_nt(widen_cols(both, w_in.shape[1]), w_in), both, hidden


def put_rows(send, part, at):
    rows = part.shape[0] // send.shape[0]
    for t in range(send.shape[0]):
        send[t, at : at + rows, :] = part[t * rows : (t + 1) * rows].astype(bf16)


def get_rows(whole, got, at):
    rows = whole.shape[0] // got.shape[0]
    for t in range(got.shape[0]):
        whole[t * rows : (t + 1) * rows, :] = got[t, at : at + rows, :]


def padded(n):
    return -(-n // 128) * 128


def sum_rows(got, at, rows):
    total = got[0, at : at + rows, :].astype(f32)
    for t in range(1, got.shape[0]):
        total = total + got[t, at : at + rows, :].astype(f32)
    return total


def forward_rows(late, branch):
    return (late.astype(f32) + 0.5 * branch).astype(bf16)


def backward_rows(early, cot, gain, normed_grad):
    widened = early.astype(f32)
    factor = row_factor(widened)
    scaled = normed_grad * gain
    unit = widened * factor
    mean = jnp.mean(scaled * unit, axis=-1, keepdims=True)
    return (cot.astype(f32) + factor * (scaled - unit * mean)).astype(bf16)


def start_copies(pairs, sems):
    copies = [pltpu.make_async_copy(a, b, sems.at[k]) for k, (a, b) in enumerate(pairs)]
    for copy in copies:
        copy.start()
    return copies


def weights_of(w, h, block):
    split = padded(2 * h)
    start = block * (split + padded(h))
    return w.at[:, start : start + split], w.at[:, start + split : start + split + padded(h)]


def stage_one(
    h, late, early, cot, gain_1, gain_2, w, send, normed, both, hidden,
    v_in, v_down, v_in_1, v_down_1, v_early, v_cot, v_late, sems,
):
    w_in, w_down = weights_of(w, h, 1)
    w_in_1, w_down_1 = weights_of(w, h, 0)
    copies = start_copies(
        (
            (early, v_early), (w_in, v_in), (cot, v_cot), (w_down, v_down),
            (late, v_late), (w_in_1, v_in_1), (w_down_1, v_down_1),
        ),
        sems,
    )
    copies[0].wait()
    saved = normalize(v_early[...], gain_2[...])
    normed[...] = saved
    copies[1].wait()
    pre = dot_nn(saved, v_in[...])
    copies[2].wait()
    copies[3].wait()
    part, both[...], hidden[...] = backward_part(pre, v_cot[...], v_in[...], v_down[...], h)
    put_rows(send, part, send.shape[1] // 2)
    for copy in copies[4:]:
        copy.wait()
    rows = normalize(v_late[...], gain_1[...])
    put_rows(send, forward_part(rows, v_in_1[...], v_down_1[...], h), 0)


def recompute(h, early, gain, w, normed, pre, v_in, v_early, sems):
    copies = start_copies(((early, v_early), (weights_of(w, h, 0)[0], v_in)), sems)
    copies[0].wait()
    rows = normalize(v_early[...], gain[...])
    normed[...] = rows
    copies[1].wait()
    pre[...] = dot_nn(rows, v_in[...])


def backward_first(h, got, pre, w, cot, other, both, hidden, v_in, v_down, sems):
    w_in, w_down = weights_of(w, h, 0)
    copies = start_copies(((w_down, v_down), (w_in, v_in)), sems)
    get_rows(cot, got, got.shape[1] // 2)
    for copy in copies:
        copy.wait()
    part, both[...], hidden[...] = backward_part(pre[...], cot[...], v_in[...], v_down[...], h)
    put_rows(other, part, 0)


def forward_second(h, got, other, gain, w, late, send, v_in, v_down, sems):
    w_in, w_down = weights_of(w, h, 1)
    copies = start_copies(((w_in, v_in), (w_down, v_down)), sems)
    get_rows(late, got, 0)
    normed = normalize(late[...], gain[...])
    rows = other.shape[1]
    for t in range(send.shape[0]):
        send[t, rows:, :] = other[t]
    for copy in copies:
        copy.wait()
    put_rows(send, forward_part(normed, v_in[...], v_down[...], h), 0)


def update_rows(got, late, early, cot, gain, send, own):
    rows = late.shape[0]
    own[:rows, :] = forward_rows(late[...], sum_rows(got, 0, rows))
    own[rows:, :] = backward_rows(early[...], cot[...], gain[...], sum_rows(got, rows, rows))
    for t in range(send.shape[0]):
        send[t] = own[...]


def pair_sum(mine, got, out):
    for z in range(out.shape[0]):
        out[z] = (mine[z].astype(f32) + got[z].astype(f32)).astype(bf16)


def near_parts(place, mine, got, *outs):
    for k in range(outs[0].shape[0]):
        for step, out in enumerate(outs):
            at = 4 * k + place[step]
            out[k] = (mine[at].astype(f32) + got[at].astype(f32)).astype(bf16)


def far_parts(place, own, one, back, two, *refs):
    outs, scratch = refs[:-1], refs[-1]
    for k in range(own.shape[0]):
        scratch[k] = (
            own[k].astype(f32) + one[k].astype(f32) + back[k].astype(f32) + two[k].astype(f32)
        ).astype(bf16)
    for step, out in enumerate(outs):
        out[...] = scratch[place[step]]


def add_gradients(h, here, near, far, second, *refs):
    sums, outs = refs[:6], refs[6:]
    first = here[...].astype(f32) + near[...].astype(f32) + far[...].astype(f32)
    for block, grads in enumerate((first, second[...].astype(f32))):
        for k in range(3):
            outs[3 * block + k][...] = sums[3 * block + k][...] + grads[:, k * h : (k + 1) * h]


def pack_weights(*refs):
    out, held, sems = refs[6], refs[7:13], refs[13]
    rows, h = refs[0].shape
    for copy in start_copies(tuple(zip(refs[:6], held)), sems):
        copy.wait()
    pad_in, pad_down = padded(2 * h) - 2 * h, padded(h) - h
    parts = []
    for gate, up, down in (held[:3], held[3:]):
        zeros = jnp.zeros((rows, pad_in + pad_down), bf16)
        parts += [gate[...], up[...], zeros[:, :pad_in], down[...], zeros[:, :pad_down]]
    out[...] = jnp.concatenate(parts, axis=1)


def block_products(normed, both, hidden, cot, z, size):
    cols = slice(z * size, (z + 1) * size)
    return dot_tn(normed[:, cols], both[...]), 0.5 * dot_tn(cot[:, cols], hidden[...])


def weight_parts_by_core(core, normed, both, hidden, cot, mine, theirs):
    rows, wide = mine.shape[1], both.shape[1]
    first = core[0] == 0
    for z in range(mine.shape[0]):
        for part, cols in zip(
            block_products(normed, both, hidden, cot, z, 2 * rows),
            (slice(0, wide), slice(wide, mine.shape[2])),
        ):
            top, bottom = part[:rows], part[rows:]
            mine[z, :, cols] = jnp.where(first, top, bottom).astype(bf16)
            theirs[z, :, cols] = jnp.where(first, bottom, top).astype(bf16)


def call(body, outs, *args, scalars=0, scratch=(), copied=()):
    spaces = [
        pltpu.SMEM if k < scalars else pltpu.HBM if k in copied else pltpu.VMEM
        for k in range(len(args))
    ]
    sems = [pltpu.SemaphoreType.DMA((len(scratch),))] if copied else []
    return pl.pallas_call(
        body,
        in_specs=[pl.BlockSpec(memory_space=space) for space in spaces],
        out_specs=[pl.BlockSpec(memory_space=pltpu.VMEM)] * len(outs),
        out_shape=[
            jax.ShapeDtypeStruct(shape[:-1], f32)
            if shape[-1] is f32
            else jax.ShapeDtypeStruct(shape, bf16)
            for shape in outs
        ],
        scratch_shapes=[pltpu.VMEM(shape, bf16) for shape in scratch] + sems,
        compiler_params=pltpu.CompilerParams(vmem_limit_bytes=48 * 2**20),
    )(*(
        pltpu.with_memory_space_constraint(a, pltpu.HBM) if k in copied else a
        for k, a in enumerate(args)
    ))


def own_rows(a):
    rows = a.shape[0] // lax.axis_size("tp")
    return lax.dynamic_slice_in_dim(a, lax.axis_index("tp") * rows, rows, axis=0)


def exchange(a):
    return lax.all_to_all(a, "tp", split_axis=0, concat_axis=0, tiled=True)


def moved(a, step, mirror=False):
    n = lax.axis_size("fs")
    sign = [1, -1 if mirror else 1]
    return lax.ppermute(a, "fs", [(q, (q + 2 * step * sign[q % 2]) % n) for q in range(n)])


def swapped(a):
    n = lax.axis_size("fs")
    return lax.ppermute(a, "fs", [(q, q ^ 1) for q in range(n)])


def swapped_parts(core, saved, cot, n_fs, d, h):
    block = (n_fs // 2, d // n_fs, 3 * h)
    mine, theirs = call(weight_parts_by_core, (block, block), core, *saved, cot, scalars=1)
    return mine, swapped(theirs)


def reduce_offloaded(mine, got):
    n = lax.axis_size("fs")
    groups = [[2 * z + c for z in range(n // 2)] for c in range(2)]
    (pair,) = call(pair_sum, (mine.shape,), mine, got)
    return lax.psum_scatter(
        pair.reshape(-1, pair.shape[2]), "fs",
        scatter_dimension=0, tiled=True, axis_index_groups=groups,
    )


def near_level(core, z, mine, got):
    steps = (0, 1, -1, -2)
    classes = jnp.stack([(z + step * (1 - 2 * core)) % 4 for step in steps]).astype(jnp.int32)
    own, *parts = call(
        near_parts, ((4,) + mine.shape[1:],) * 4, classes, mine, got, scalars=1
    )
    return own, *(moved(part, step, mirror=True) for part, step in zip(parts, steps[1:]))


def far_level(core, kz, *parts):
    block = parts[0].shape
    sign = 1 - 2 * core
    place = jnp.stack([(kz + step) % 4 for step in (0, sign, 2, -sign)]).astype(jnp.int32)
    here, on, across, back = call(
        far_parts, (block[1:],) * 4, place, *parts, scalars=1, scratch=(block,)
    )
    across = moved(across, 4, mirror=True)
    back = moved(back, -4, mirror=True)
    on = (on.astype(f32) + across.astype(f32)).astype(bf16)
    return here, moved(on, 4, mirror=True), back


def per_device(
    late_input,
    early_input,
    early_mid,
    cotangent,
    gain_first,
    gain_second,
    gate_first,
    up_first,
    down_first,
    gate_second,
    up_second,
    down_second,
    sum_gate_first,
    sum_up_first,
    sum_down_first,
    sum_gate_second,
    sum_up_second,
    sum_down_second,
):
    h = gate_first.shape[1]
    tokens, d = late_input.shape
    n = lax.axis_size("tp")
    n_fs = lax.axis_size("fs")
    rows = tokens // n
    gain_1, gain_2 = gain_first[None], gain_second[None]
    index = lax.axis_index("fs").astype(jnp.int32)
    core = (index % 2).astype(jnp.int32)[None]
    late_own, early_own, mid_own, cot_own = (
        own_rows(a) for a in (late_input, early_input, early_mid, cotangent)
    )
    wide = 2 * (padded(2 * h) + padded(h))
    (packed,) = call(
        pack_weights, ((gate_first.shape[0], wide),),
        gate_first, up_first, down_first.T, gate_second, up_second, down_second.T,
        copied=tuple(range(6)), scratch=(gate_first.shape,) * 6,
    )
    w = lax.all_gather(packed, "fs", axis=0, tiled=True)

    double, whole = (n, 2 * rows, d), (tokens, d)
    saved_shapes = (whole, (tokens, 2 * h), (tokens, h))
    held = ((d, padded(2 * h)), (d, padded(h)))
    send, *saved_second = call(
        lambda *refs: stage_one(h, *refs), (double,) + saved_shapes,
        late_input, early_mid, cotangent, gain_1, gain_2, w,
        copied=(0, 1, 2, 5), scratch=held + held + (whole,) * 3,
    )
    got = exchange(send)
    pieces_2 = swapped_parts(core, saved_second, cotangent, n_fs, d, h)
    normed, pre = call(
        lambda *refs: recompute(h, *refs), (whole, (tokens, padded(2 * h), f32)),
        early_input, gain_1, w, copied=(0, 2), scratch=held[:1] + (whole,),
    )
    send, own = call(
        update_rows, (double, (2 * rows, d)), got, late_own, mid_own, cot_own, gain_2
    )
    got = exchange(send)
    g2 = reduce_offloaded(*pieces_2)

    mid_grad, other, *saved_first = call(
        lambda *refs: backward_first(h, *refs), (whole, (n, rows, d)) + saved_shapes[1:],
        got, pre, w, copied=(2,), scratch=held,
    )
    late_mid, send = call(
        lambda *refs: forward_second(h, *refs), (whole, double),
        got, other, gain_2, w, copied=(3,), scratch=held,
    )
    got = exchange(send)
    pieces_1 = swapped_parts(core, (normed, *saved_first), mid_grad, n_fs, d, h)
    near = near_level(core[0], index // 2, *pieces_1)
    send, _ = call(
        update_rows, (double, (2 * rows, d)), got, own[:rows], early_own, own[rows:], gain_1
    )
    got = exchange(send)
    pieces = far_level(core[0], index // 8, *near)
    late_out = got[:, :rows].reshape(whole)
    input_grad = got[:, rows:].reshape(whole)
    sums = call(
        lambda *refs: add_gradients(h, *refs), (gate_first.shape + (f32,),) * 6, *pieces, g2,
        sum_gate_first, sum_up_first, sum_down_first.T,
        sum_gate_second, sum_up_second, sum_down_second.T,
    )
    return (
        late_mid, late_out, input_grad,
        sums[0], sums[1], sums[2].T, sums[3], sums[4], sums[5].T,
    )


def solution(mesh):
    rows, w_in, w_out = P("fs", None), P("fs", "tp"), P("tp", "fs")
    weights = (w_in, w_in, w_out) * 2

    return jax.shard_map(
        per_device,
        mesh=mesh,
        in_specs=(rows,) * 4 + (P(), P()) + weights + weights,
        out_specs=(rows,) * 3 + weights,
        check_vma=False,
    )
```

```python
import jax
import jax.numpy as jnp
from jax import lax
from jax.experimental import pallas as pl
from jax.experimental.pallas import tpu as pltpu
from jax.sharding import PartitionSpec as P

norm_eps = 1e-06
f32, bf16 = jnp.float32, jnp.bfloat16


def dot_nn(a, b):
    return jnp.dot(a, b, preferred_element_type=f32)


def dot_nt(a, b):
    return lax.dot_general(a, b, (((1,), (1,)), ((), ())), preferred_element_type=f32)


def dot_tn(a, b):
    return lax.dot_general(a, b, (((0,), (0,)), ((), ())), preferred_element_type=f32)


def row_factor(widened):
    return lax.rsqrt(jnp.mean(widened * widened, axis=-1, keepdims=True) + norm_eps)


def normalize(values, gain):
    widened = values.astype(f32)
    return (widened * row_factor(widened) * gain).astype(bf16)


def widen_cols(a, width):
    return jnp.concatenate([a, jnp.zeros((a.shape[0], width - a.shape[1]), a.dtype)], axis=1)


def forward_part(normed, w_in, w_down, h):
    pre = dot_nn(normed, w_in)
    gate, up = pre[:, :h], pre[:, h : 2 * h]
    hidden = (gate * jax.nn.sigmoid(gate) * up).astype(bf16)
    return dot_nt(widen_cols(hidden, w_down.shape[1]), w_down)


def backward_part(pre, cot, w_in, w_down, h):
    gate, up = pre[:, :h], pre[:, h : 2 * h]
    s = jax.nn.sigmoid(gate)
    activated = gate * s
    hidden = (activated * up).astype(bf16)
    hidden_grad = 0.5 * dot_nn(cot, w_down)[:, :h]
    gate_grad = hidden_grad * up * s * (1.0 + gate * (1.0 - s))
    both = jnp.concatenate([gate_grad, hidden_grad * activated], axis=1).astype(bf16)
    return dot_nt(widen_cols(both, w_in.shape[1]), w_in), both, hidden


def put_rows(send, part, at):
    rows = part.shape[0] // send.shape[0]
    for t in range(send.shape[0]):
        send[t, at : at + rows, :] = part[t * rows : (t + 1) * rows].astype(bf16)


def get_rows(whole, got, at):
    rows = whole.shape[0] // got.shape[0]
    for t in range(got.shape[0]):
        whole[t * rows : (t + 1) * rows, :] = got[t, at : at + rows, :]


def padded(n):
    return -(-n // 128) * 128


def sum_rows(got, at, rows):
    total = got[0, at : at + rows, :].astype(f32)
    for t in range(1, got.shape[0]):
        total = total + got[t, at : at + rows, :].astype(f32)
    return total


def forward_rows(late, branch):
    return (late.astype(f32) + 0.5 * branch).astype(bf16)


def backward_rows(early, cot, gain, normed_grad):
    widened = early.astype(f32)
    factor = row_factor(widened)
    scaled = normed_grad * gain
    unit = widened * factor
    mean = jnp.mean(scaled * unit, axis=-1, keepdims=True)
    return (cot.astype(f32) + factor * (scaled - unit * mean)).astype(bf16)


def start_copies(pairs, sems, first=0):
    copies = [pltpu.make_async_copy(a, b, sems.at[first + k]) for k, (a, b) in enumerate(pairs)]
    for copy in copies:
        copy.start()
    return copies


def weights_of(w, h, block):
    split = padded(2 * h)
    start = block * (split + padded(h))
    return w.at[:, start : start + split], w.at[:, start + split : start + split + padded(h)]


def prepare(at, late, early, mid, cot, gain_1, gain_2, *refs):
    normed, own, held, sems = refs[:3], refs[3:7], refs[7:12], refs[12]
    rows = own[0].shape[0]
    mine = pl.ds(pl.multiple_of(at[0] * rows, rows), rows)
    copies = start_copies(
        (*zip((late, early, mid, gain_1, gain_2), held),
         *((a.at[mine], out) for a, out in zip((late, early, mid, cot), own))),
        sems,
    )
    for copy in copies:
        copy.wait()
    for values, gain, out in zip(held[:3], (held[3], held[3], held[4]), normed):
        out[...] = normalize(values[...], gain[...])


def stage_one(
    h, late, early, cot, w, send, both, hidden,
    v_in, v_down, v_in_1, v_down_1, v_cot, v_b, v_f, sems,
):
    w_in, w_down = weights_of(w, h, 1)
    w_in_1, w_down_1 = weights_of(w, h, 0)
    copies = start_copies(
        (
            (w_in, v_in), (cot, v_cot), (w_down, v_down),
            (w_in_1, v_in_1), (w_down_1, v_down_1),
        ),
        sems,
    )
    copies[0].wait()
    pre = dot_nn(early[...], v_in[...])
    copies[1].wait()
    copies[2].wait()
    part, both[...], hidden[...] = backward_part(pre, v_cot[...], v_in[...], v_down[...], h)
    rows = v_b.shape[1]
    put_rows(v_b, part, 0)
    outs = start_copies(((v_b, send.at[:, rows:, :]),), sems, 5)
    for copy in copies[3:]:
        copy.wait()
    put_rows(v_f, forward_part(late[...], v_in_1[...], v_down_1[...], h), 0)
    outs += start_copies(((v_f, send.at[:, :rows, :]),), sems, 6)
    for copy in outs:
        copy.wait()


def recompute(h, normed, w, pre, v_in, sems):
    (copy,) = start_copies(((weights_of(w, h, 0)[0], v_in),), sems)
    copy.wait()
    pre[...] = dot_nn(normed[...], v_in[...])


def backward_first(h, got, pre, w, cot, other, both, hidden, v_in, v_down, sems):
    w_in, w_down = weights_of(w, h, 0)
    copies = start_copies(((w_down, v_down), (w_in, v_in)), sems)
    get_rows(cot, got, got.shape[1] // 2)
    for copy in copies:
        copy.wait()
    part, both[...], hidden[...] = backward_part(pre[...], cot[...], v_in[...], v_down[...], h)
    put_rows(other, part, 0)


def forward_second(h, got, other, gain, w, late, send, v_in, v_down, v_gain, v_part, sems):
    w_in, w_down = weights_of(w, h, 1)
    rows = other.shape[1]
    copies = start_copies(
        ((gain, v_gain), (w_in, v_in), (w_down, v_down), (other, send.at[:, rows:, :])), sems
    )
    get_rows(late, got, 0)
    copies[0].wait()
    normed = normalize(late[...], v_gain[...])
    copies[1].wait()
    copies[2].wait()
    put_rows(v_part, forward_part(normed, v_in[...], v_down[...], h), 0)
    copies += start_copies(((v_part, send.at[:, :rows, :]),), sems, 4)
    copies[3].wait()
    copies[4].wait()


def update_rows(got, late, early, cot, gain, send, own, v_gain, sems):
    (copy,) = start_copies(((gain, v_gain),), sems)
    rows = late.shape[0]
    own[:rows, :] = forward_rows(late[...], sum_rows(got, 0, rows))
    copy.wait()
    own[rows:, :] = backward_rows(early[...], cot[...], v_gain[...], sum_rows(got, rows, rows))
    for copy in start_copies([(own, send.at[t]) for t in range(send.shape[0])], sems, 1):
        copy.wait()


def pair_sum(mine, got, out):
    for z in range(out.shape[0]):
        out[z] = (mine[z].astype(f32) + got[z].astype(f32)).astype(bf16)


def near_parts(place, mine, got, *outs):
    for k in range(outs[0].shape[0]):
        for step, out in enumerate(outs):
            at = 4 * k + place[step]
            out[k] = (mine[at].astype(f32) + got[at].astype(f32)).astype(bf16)


def far_parts(place, own, one, back, two, *refs):
    outs, scratch = refs[:-1], refs[-1]
    for k in range(own.shape[0]):
        scratch[k] = (
            own[k].astype(f32) + one[k].astype(f32) + back[k].astype(f32) + two[k].astype(f32)
        ).astype(bf16)
    for step, out in enumerate(outs):
        out[...] = scratch[place[step]]


def add_gradients(h, here, near, far, second, *refs):
    sums, outs, v_second, sems = refs[:6], refs[6:12], refs[12], refs[13]
    (copy,) = start_copies(((second, v_second),), sems)
    copy.wait()
    first = here[...].astype(f32) + near[...].astype(f32) + far[...].astype(f32)
    for block, grads in enumerate((first, v_second[...].astype(f32))):
        for k in range(3):
            outs[3 * block + k][...] = sums[3 * block + k][...] + grads[:, k * h : (k + 1) * h]


def pack_weights(*refs):
    out, held, sems = refs[6], refs[7:13], refs[13]
    rows, h = refs[0].shape
    for copy in start_copies(tuple(zip(refs[:6], held)), sems):
        copy.wait()
    pad_in, pad_down = padded(2 * h) - 2 * h, padded(h) - h
    parts = []
    for gate, up, down in (held[:3], held[3:]):
        zeros = jnp.zeros((rows, pad_in + pad_down), bf16)
        parts += [gate[...], up[...], zeros[:, :pad_in], down[...], zeros[:, :pad_down]]
    out[...] = jnp.concatenate(parts, axis=1)


def block_products(normed, both, hidden, cot, z, size):
    cols = slice(z * size, (z + 1) * size)
    return dot_tn(normed[:, cols], both[...]), 0.5 * dot_tn(cot[:, cols], hidden[...])


def weight_parts_by_core(core, normed, both, hidden, cot, mine, theirs):
    rows, wide = mine.shape[1], both.shape[1]
    first = core[0] == 0
    for z in range(mine.shape[0]):
        for part, cols in zip(
            block_products(normed, both, hidden, cot, z, 2 * rows),
            (slice(0, wide), slice(wide, mine.shape[2])),
        ):
            top, bottom = part[:rows], part[rows:]
            mine[z, :, cols] = jnp.where(first, top, bottom).astype(bf16)
            theirs[z, :, cols] = jnp.where(first, bottom, top).astype(bf16)


def call(body, outs, *args, scalars=0, scratch=(), copied=(), copies=None):
    def typed(shape):
        return (shape[:-1], f32) if shape[-1] is f32 else (shape, bf16)

    def result(shape):
        if shape[-1] is pltpu.HBM:
            return pltpu.HBM(shape[:-1], bf16)
        return jax.ShapeDtypeStruct(*typed(shape))

    spaces = [
        pltpu.SMEM if k < scalars else pltpu.HBM if k in copied else pltpu.VMEM
        for k in range(len(args))
    ]
    sems = [pltpu.SemaphoreType.DMA((copies or len(scratch),))] if copied else []
    return pl.pallas_call(
        body,
        in_specs=[pl.BlockSpec(memory_space=space) for space in spaces],
        out_specs=[
            pl.BlockSpec(memory_space=pltpu.HBM if shape[-1] is pltpu.HBM else pltpu.VMEM)
            for shape in outs
        ],
        out_shape=[result(shape) for shape in outs],
        scratch_shapes=[pltpu.VMEM(*typed(shape)) for shape in scratch] + sems,
        compiler_params=pltpu.CompilerParams(vmem_limit_bytes=48 * 2**20),
    )(*(
        pltpu.with_memory_space_constraint(a, pltpu.HBM) if k in copied else a
        for k, a in enumerate(args)
    ))


def exchange(a):
    return lax.all_to_all(a, "tp", split_axis=0, concat_axis=0, tiled=True)


def moved(a, step, mirror=False):
    n = lax.axis_size("fs")
    sign = [1, -1 if mirror else 1]
    return lax.ppermute(a, "fs", [(q, (q + 2 * step * sign[q % 2]) % n) for q in range(n)])


def swapped(a):
    n = lax.axis_size("fs")
    return lax.ppermute(a, "fs", [(q, q ^ 1) for q in range(n)])


def swapped_parts(core, saved, cot, n_fs, d, h):
    block = (n_fs // 2, d // n_fs, 3 * h)
    mine, theirs = call(weight_parts_by_core, (block, block), core, *saved, cot, scalars=1)
    return mine, swapped(theirs)


def reduce_offloaded(mine, got):
    n = lax.axis_size("fs")
    groups = [[2 * z + c for z in range(n // 2)] for c in range(2)]
    (pair,) = call(pair_sum, (mine.shape,), mine, got)
    return lax.psum_scatter(
        pair.reshape(-1, pair.shape[2]), "fs",
        scatter_dimension=0, tiled=True, axis_index_groups=groups,
    )


def near_level(core, z, mine, got):
    steps = (0, 1, -1, -2)
    classes = jnp.stack([(z + step * (1 - 2 * core)) % 4 for step in steps]).astype(jnp.int32)
    own, *parts = call(
        near_parts, ((4,) + mine.shape[1:],) * 4, classes, mine, got, scalars=1
    )
    return own, *(moved(part, step, mirror=True) for part, step in zip(parts, steps[1:]))


def far_level(core, kz, *parts):
    block = parts[0].shape
    sign = 1 - 2 * core
    place = jnp.stack([(kz + step) % 4 for step in (0, sign, 2, -sign)]).astype(jnp.int32)
    here, on, across, back = call(
        far_parts, (block[1:],) * 4, place, *parts, scalars=1, scratch=(block,)
    )
    across = moved(across, 4, mirror=True)
    back = moved(back, -4, mirror=True)
    on = (on.astype(f32) + across.astype(f32)).astype(bf16)
    return here, moved(on, 4, mirror=True), back


def per_device(
    late_input,
    early_input,
    early_mid,
    cotangent,
    gain_first,
    gain_second,
    gate_first,
    up_first,
    down_first,
    gate_second,
    up_second,
    down_second,
    sum_gate_first,
    sum_up_first,
    sum_down_first,
    sum_gate_second,
    sum_up_second,
    sum_down_second,
):
    h = gate_first.shape[1]
    tokens, d = late_input.shape
    n = lax.axis_size("tp")
    n_fs = lax.axis_size("fs")
    rows = tokens // n
    gain_1, gain_2 = gain_first[None], gain_second[None]
    index = lax.axis_index("fs").astype(jnp.int32)
    core = (index % 2).astype(jnp.int32)[None]
    wide = 2 * (padded(2 * h) + padded(h))
    (packed,) = call(
        pack_weights, ((gate_first.shape[0], wide),),
        gate_first, up_first, down_first.T, gate_second, up_second, down_second.T,
        copied=tuple(range(6)), scratch=(gate_first.shape,) * 6,
    )
    w = lax.all_gather(packed, "fs", axis=0, tiled=True)

    single, whole = (n, rows, d), (tokens, d)
    sent = (n, 2 * rows, d, pltpu.HBM)
    saved_shapes = (whole, (tokens, 2 * h), (tokens, h))
    held = ((d, padded(2 * h)), (d, padded(h)))
    gain_shape = (1, d, f32)
    normed_late, normed, normed_mid, late_own, early_own, mid_own, cot_own = call(
        prepare, (whole,) * 3 + ((rows, d),) * 4, lax.axis_index("tp").astype(jnp.int32)[None],
        late_input, early_input, early_mid, cotangent, gain_1, gain_2,
        scalars=1, copied=tuple(range(1, 7)), scratch=(whole,) * 3 + (gain_shape,) * 2, copies=9,
    )
    send, *saved_second = call(
        lambda *refs: stage_one(h, *refs), (sent,) + saved_shapes[1:],
        normed_late, normed_mid, cotangent, w,
        copied=(2, 3), scratch=held + held + (whole,) + (single,) * 2,
    )
    saved_second = (normed_mid, *saved_second)
    got = exchange(send)
    pieces_2 = swapped_parts(core, saved_second, cotangent, n_fs, d, h)
    (pre,) = call(
        lambda *refs: recompute(h, *refs), ((tokens, padded(2 * h), f32),),
        normed, w, copied=(1,), scratch=held[:1],
    )
    send, own = call(
        update_rows, (sent, (2 * rows, d)), got, late_own, mid_own, cot_own, gain_2,
        copied=(4,), scratch=(gain_shape,), copies=1 + n,
    )
    got = exchange(send)
    g2 = reduce_offloaded(*pieces_2)

    mid_grad, other, *saved_first = call(
        lambda *refs: backward_first(h, *refs), (whole, single) + saved_shapes[1:],
        got, pre, w, copied=(2,), scratch=held,
    )
    late_mid, send = call(
        lambda *refs: forward_second(h, *refs), (whole, sent),
        got, other, gain_2, w, copied=(2, 3), scratch=held + (gain_shape, single), copies=5,
    )
    got = exchange(send)
    pieces_1 = swapped_parts(core, (normed, *saved_first), mid_grad, n_fs, d, h)
    near = near_level(core[0], index // 2, *pieces_1)
    send, _ = call(
        update_rows, (sent, (2 * rows, d)), got, own[:rows], early_own, own[rows:], gain_1,
        copied=(4,), scratch=(gain_shape,), copies=1 + n,
    )
    got = exchange(send)
    pieces = far_level(core[0], index // 8, *near)
    late_out = got[:, :rows].reshape(whole)
    input_grad = got[:, rows:].reshape(whole)
    sums = call(
        lambda *refs: add_gradients(h, *refs), (gate_first.shape + (f32,),) * 6, *pieces, g2,
        sum_gate_first, sum_up_first, sum_down_first.T,
        sum_gate_second, sum_up_second, sum_down_second.T,
        copied=(3,), scratch=(g2.shape,),
    )
    return (
        late_mid, late_out, input_grad,
        sums[0], sums[1], sums[2].T, sums[3], sums[4], sums[5].T,
    )


def solution(mesh):
    rows, w_in, w_out = P("fs", None), P("fs", "tp"), P("tp", "fs")
    weights = (w_in, w_in, w_out) * 2

    return jax.shard_map(
        per_device,
        mesh=mesh,
        in_specs=(rows,) * 4 + (P(), P()) + weights + weights,
        out_specs=(rows,) * 3 + weights,
        check_vma=False,
    )
```

```python
import jax
import jax.numpy as jnp
from jax import lax
from jax.experimental import pallas as pl
from jax.experimental.pallas import tpu as pltpu
from jax.sharding import PartitionSpec as P

norm_eps = 1e-06
f32, bf16 = jnp.float32, jnp.bfloat16


def dot_nn(a, b):
    return jnp.dot(a, b, preferred_element_type=f32)


def dot_nt(a, b):
    return lax.dot_general(a, b, (((1,), (1,)), ((), ())), preferred_element_type=f32)


def dot_tn(a, b):
    return lax.dot_general(a, b, (((0,), (0,)), ((), ())), preferred_element_type=f32)


def row_factor(widened):
    return lax.rsqrt(jnp.mean(widened * widened, axis=-1, keepdims=True) + norm_eps)


def normalize(values, gain):
    widened = values.astype(f32)
    return (widened * row_factor(widened) * gain).astype(bf16)


def widen_cols(a, width):
    return jnp.concatenate([a, jnp.zeros((a.shape[0], width - a.shape[1]), a.dtype)], axis=1)


def forward_part(normed, w_in, w_down, h):
    pre = dot_nn(normed, w_in)
    gate, up = pre[:, :h], pre[:, h : 2 * h]
    hidden = (gate * jax.nn.sigmoid(gate) * up).astype(bf16)
    return dot_nt(widen_cols(hidden, w_down.shape[1]), w_down)


def backward_part(pre, cot, w_in, w_down, h):
    gate, up = pre[:, :h], pre[:, h : 2 * h]
    s = jax.nn.sigmoid(gate)
    activated = gate * s
    hidden = (activated * up).astype(bf16)
    hidden_grad = 0.5 * dot_nn(cot, w_down)[:, :h]
    gate_grad = hidden_grad * up * s * (1.0 + gate * (1.0 - s))
    both = jnp.concatenate([gate_grad, hidden_grad * activated], axis=1).astype(bf16)
    return dot_nt(widen_cols(both, w_in.shape[1]), w_in), both, hidden


def put_rows(send, part, at):
    rows = part.shape[0] // send.shape[0]
    for t in range(send.shape[0]):
        send[t, at : at + rows, :] = part[t * rows : (t + 1) * rows].astype(bf16)


def get_rows(whole, got, at):
    rows = whole.shape[0] // got.shape[0]
    for t in range(got.shape[0]):
        whole[t * rows : (t + 1) * rows, :] = got[t, at : at + rows, :]


def padded(n):
    return -(-n // 128) * 128


def sum_rows(got, at, rows):
    total = got[0, at : at + rows, :].astype(f32)
    for t in range(1, got.shape[0]):
        total = total + got[t, at : at + rows, :].astype(f32)
    return total


def forward_rows(late, branch):
    return (late.astype(f32) + 0.5 * branch).astype(bf16)


def backward_rows(early, cot, gain, normed_grad):
    widened = early.astype(f32)
    factor = row_factor(widened)
    scaled = normed_grad * gain
    unit = widened * factor
    mean = jnp.mean(scaled * unit, axis=-1, keepdims=True)
    return (cot.astype(f32) + factor * (scaled - unit * mean)).astype(bf16)


def start_copies(pairs, sems, first=0):
    copies = [pltpu.make_async_copy(a, b, sems.at[first + k]) for k, (a, b) in enumerate(pairs)]
    for copy in copies:
        copy.start()
    return copies


def weights_of(w, h, block):
    split = padded(2 * h)
    start = block * (split + padded(h))
    return w.at[:, start : start + split], w.at[:, start + split : start + split + padded(h)]


def prepare(at, late, early, mid, cot, gain_1, gain_2, *refs):
    normed, own, held, sems = refs[:3], refs[3:7], refs[7:12], refs[12]
    rows = own[0].shape[0]
    mine = pl.ds(pl.multiple_of(at[0] * rows, rows), rows)
    copies = start_copies(
        (*zip((late, early, mid, gain_1, gain_2), held),
         *((a.at[mine], out) for a, out in zip((late, early, mid, cot), own))),
        sems,
    )
    for copy in copies:
        copy.wait()
    for values, gain, out in zip(held[:3], (held[3], held[3], held[4]), normed):
        out[...] = normalize(values[...], gain[...])


def stage_one(
    h, late, early, cot, w, send, both, hidden,
    v_in, v_down, v_in_1, v_down_1, v_cot, v_b, v_f, sems,
):
    w_in, w_down = weights_of(w, h, 1)
    w_in_1, w_down_1 = weights_of(w, h, 0)
    copies = start_copies(
        (
            (w_in, v_in), (cot, v_cot), (w_down, v_down),
            (w_in_1, v_in_1), (w_down_1, v_down_1),
        ),
        sems,
    )
    copies[0].wait()
    pre = dot_nn(early[...], v_in[...])
    copies[1].wait()
    copies[2].wait()
    part, both[...], hidden[...] = backward_part(pre, v_cot[...], v_in[...], v_down[...], h)
    rows = v_b.shape[1]
    put_rows(v_b, part, 0)
    outs = start_copies(((v_b, send.at[:, rows:, :]),), sems, 5)
    for copy in copies[3:]:
        copy.wait()
    put_rows(v_f, forward_part(late[...], v_in_1[...], v_down_1[...], h), 0)
    outs += start_copies(((v_f, send.at[:, :rows, :]),), sems, 6)
    for copy in outs:
        copy.wait()


def recompute(h, normed, w, pre, v_in, sems):
    (copy,) = start_copies(((weights_of(w, h, 0)[0], v_in),), sems)
    copy.wait()
    pre[...] = dot_nn(normed[...], v_in[...])


def backward_first(h, got, pre, w, cot, other, both, hidden, v_in, v_down, sems):
    w_in, w_down = weights_of(w, h, 0)
    copies = start_copies(((w_down, v_down), (w_in, v_in)), sems)
    get_rows(cot, got, got.shape[1] // 2)
    for copy in copies:
        copy.wait()
    part, both[...], hidden[...] = backward_part(pre[...], cot[...], v_in[...], v_down[...], h)
    put_rows(other, part, 0)


def forward_second(h, got, other, gain, w, late, send, v_in, v_down, v_gain, v_send, sems):
    w_in, w_down = weights_of(w, h, 1)
    rows = other.shape[1]
    copies = start_copies(((gain, v_gain), (w_in, v_in), (w_down, v_down)), sems)
    get_rows(late, got, 0)
    copies[0].wait()
    normed = normalize(late[...], v_gain[...])
    for t in range(v_send.shape[0]):
        v_send[t, rows:, :] = other[t]
    copies[1].wait()
    copies[2].wait()
    put_rows(v_send, forward_part(normed, v_in[...], v_down[...], h), 0)
    (copy,) = start_copies(((v_send, send),), sems, 3)
    copy.wait()


def update_rows(got, late, early, cot, gain, send, own, v_gain, v_send, sems):
    (copy,) = start_copies(((gain, v_gain),), sems)
    rows = late.shape[0]
    own[:rows, :] = forward_rows(late[...], sum_rows(got, 0, rows))
    copy.wait()
    own[rows:, :] = backward_rows(early[...], cot[...], v_gain[...], sum_rows(got, rows, rows))
    for t in range(v_send.shape[0]):
        v_send[t] = own[...]
    (copy,) = start_copies(((v_send, send),), sems, 1)
    copy.wait()


def pair_sum(mine, got, out):
    for z in range(out.shape[0]):
        out[z] = (mine[z].astype(f32) + got[z].astype(f32)).astype(bf16)


def near_parts(place, mine, got, *outs):
    for k in range(outs[0].shape[0]):
        for step, out in enumerate(outs):
            at = 4 * k + place[step]
            out[k] = (mine[at].astype(f32) + got[at].astype(f32)).astype(bf16)


def far_parts(place, own, one, back, two, *refs):
    outs, scratch = refs[:-1], refs[-1]
    for k in range(own.shape[0]):
        scratch[k] = (
            own[k].astype(f32) + one[k].astype(f32) + back[k].astype(f32) + two[k].astype(f32)
        ).astype(bf16)
    for step, out in enumerate(outs):
        out[...] = scratch[place[step]]


def add_gradients(h, here, near, far, second, *refs):
    sums, outs, v_second, sems = refs[:6], refs[6:12], refs[12], refs[13]
    (copy,) = start_copies(((second, v_second),), sems)
    copy.wait()
    first = here[...].astype(f32) + near[...].astype(f32) + far[...].astype(f32)
    for block, grads in enumerate((first, v_second[...].astype(f32))):
        for k in range(3):
            outs[3 * block + k][...] = sums[3 * block + k][...] + grads[:, k * h : (k + 1) * h]


def pack_weights(*refs):
    out, held, sems = refs[6], refs[7:13], refs[13]
    rows, h = refs[0].shape
    for copy in start_copies(tuple(zip(refs[:6], held)), sems):
        copy.wait()
    pad_in, pad_down = padded(2 * h) - 2 * h, padded(h) - h
    parts = []
    for gate, up, down in (held[:3], held[3:]):
        zeros = jnp.zeros((rows, pad_in + pad_down), bf16)
        parts += [gate[...], up[...], zeros[:, :pad_in], down[...], zeros[:, :pad_down]]
    out[...] = jnp.concatenate(parts, axis=1)


def block_products(normed, both, hidden, cot, z, size):
    cols = slice(z * size, (z + 1) * size)
    return dot_tn(normed[:, cols], both[...]), 0.5 * dot_tn(cot[:, cols], hidden[...])


def weight_parts_by_core(core, normed, both, hidden, cot, mine, theirs):
    rows, wide = mine.shape[1], both.shape[1]
    first = core[0] == 0
    for z in range(mine.shape[0]):
        for part, cols in zip(
            block_products(normed, both, hidden, cot, z, 2 * rows),
            (slice(0, wide), slice(wide, mine.shape[2])),
        ):
            top, bottom = part[:rows], part[rows:]
            mine[z, :, cols] = jnp.where(first, top, bottom).astype(bf16)
            theirs[z, :, cols] = jnp.where(first, bottom, top).astype(bf16)


def call(body, outs, *args, scalars=0, scratch=(), copied=(), copies=None):
    def typed(shape):
        return (shape[:-1], f32) if shape[-1] is f32 else (shape, bf16)

    def result(shape):
        if shape[-1] is pltpu.HBM:
            return pltpu.HBM(shape[:-1], bf16)
        return jax.ShapeDtypeStruct(*typed(shape))

    spaces = [
        pltpu.SMEM if k < scalars else pltpu.HBM if k in copied else pltpu.VMEM
        for k in range(len(args))
    ]
    sems = [pltpu.SemaphoreType.DMA((copies or len(scratch),))] if copied else []
    return pl.pallas_call(
        body,
        in_specs=[pl.BlockSpec(memory_space=space) for space in spaces],
        out_specs=[
            pl.BlockSpec(memory_space=pltpu.HBM if shape[-1] is pltpu.HBM else pltpu.VMEM)
            for shape in outs
        ],
        out_shape=[result(shape) for shape in outs],
        scratch_shapes=[pltpu.VMEM(*typed(shape)) for shape in scratch] + sems,
        compiler_params=pltpu.CompilerParams(vmem_limit_bytes=48 * 2**20),
    )(*(
        pltpu.with_memory_space_constraint(a, pltpu.HBM) if k in copied else a
        for k, a in enumerate(args)
    ))


def exchange(a):
    return lax.all_to_all(a, "tp", split_axis=0, concat_axis=0, tiled=True)


def moved(a, step, mirror=False):
    n = lax.axis_size("fs")
    sign = [1, -1 if mirror else 1]
    return lax.ppermute(a, "fs", [(q, (q + 2 * step * sign[q % 2]) % n) for q in range(n)])


def swapped(a):
    n = lax.axis_size("fs")
    return lax.ppermute(a, "fs", [(q, q ^ 1) for q in range(n)])


def swapped_parts(core, saved, cot, n_fs, d, h):
    block = (n_fs // 2, d // n_fs, 3 * h)
    mine, theirs = call(weight_parts_by_core, (block, block), core, *saved, cot, scalars=1)
    return mine, swapped(theirs)


def reduce_offloaded(mine, got):
    n = lax.axis_size("fs")
    groups = [[2 * z + c for z in range(n // 2)] for c in range(2)]
    (pair,) = call(pair_sum, (mine.shape,), mine, got)
    return lax.psum_scatter(
        pair.reshape(-1, pair.shape[2]), "fs",
        scatter_dimension=0, tiled=True, axis_index_groups=groups,
    )


def near_level(core, z, mine, got):
    steps = (0, 1, -1, -2)
    classes = jnp.stack([(z + step * (1 - 2 * core)) % 4 for step in steps]).astype(jnp.int32)
    own, *parts = call(
        near_parts, ((4,) + mine.shape[1:],) * 4, classes, mine, got, scalars=1
    )
    return own, *(moved(part, step, mirror=True) for part, step in zip(parts, steps[1:]))


def far_level(core, kz, *parts):
    block = parts[0].shape
    sign = 1 - 2 * core
    place = jnp.stack([(kz + step) % 4 for step in (0, sign, 2, -sign)]).astype(jnp.int32)
    here, on, across, back = call(
        far_parts, (block[1:],) * 4, place, *parts, scalars=1, scratch=(block,)
    )
    across = moved(across, 4, mirror=True)
    back = moved(back, -4, mirror=True)
    on = (on.astype(f32) + across.astype(f32)).astype(bf16)
    return here, moved(on, 4, mirror=True), back


def per_device(
    late_input,
    early_input,
    early_mid,
    cotangent,
    gain_first,
    gain_second,
    gate_first,
    up_first,
    down_first,
    gate_second,
    up_second,
    down_second,
    sum_gate_first,
    sum_up_first,
    sum_down_first,
    sum_gate_second,
    sum_up_second,
    sum_down_second,
):
    h = gate_first.shape[1]
    tokens, d = late_input.shape
    n = lax.axis_size("tp")
    n_fs = lax.axis_size("fs")
    rows = tokens // n
    gain_1, gain_2 = gain_first[None], gain_second[None]
    index = lax.axis_index("fs").astype(jnp.int32)
    core = (index % 2).astype(jnp.int32)[None]
    wide = 2 * (padded(2 * h) + padded(h))
    (packed,) = call(
        pack_weights, ((gate_first.shape[0], wide),),
        gate_first, up_first, down_first.T, gate_second, up_second, down_second.T,
        copied=tuple(range(6)), scratch=(gate_first.shape,) * 6,
    )
    w = lax.all_gather(packed, "fs", axis=0, tiled=True)

    single, whole = (n, rows, d), (tokens, d)
    sent = (n, 2 * rows, d, pltpu.HBM)
    saved_shapes = (whole, (tokens, 2 * h), (tokens, h))
    held = ((d, padded(2 * h)), (d, padded(h)))
    gain_shape = (1, d, f32)
    normed_late, normed, normed_mid, late_own, early_own, mid_own, cot_own = call(
        prepare, (whole,) * 3 + ((rows, d),) * 4, lax.axis_index("tp").astype(jnp.int32)[None],
        late_input, early_input, early_mid, cotangent, gain_1, gain_2,
        scalars=1, copied=tuple(range(1, 7)), scratch=(whole,) * 3 + (gain_shape,) * 2, copies=9,
    )
    send, *saved_second = call(
        lambda *refs: stage_one(h, *refs), (sent,) + saved_shapes[1:],
        normed_late, normed_mid, cotangent, w,
        copied=(2, 3), scratch=held + held + (whole,) + (single,) * 2,
    )
    saved_second = (normed_mid, *saved_second)
    got = exchange(send)
    pieces_2 = swapped_parts(core, saved_second, cotangent, n_fs, d, h)
    (pre,) = call(
        lambda *refs: recompute(h, *refs), ((tokens, padded(2 * h), f32),),
        normed, w, copied=(1,), scratch=held[:1],
    )
    send, own = call(
        update_rows, (sent, (2 * rows, d)), got, late_own, mid_own, cot_own, gain_2,
        copied=(4,), scratch=(gain_shape, sent[:3]),
    )
    got = exchange(send)
    g2 = reduce_offloaded(*pieces_2)

    mid_grad, other, *saved_first = call(
        lambda *refs: backward_first(h, *refs), (whole, single) + saved_shapes[1:],
        got, pre, w, copied=(2,), scratch=held,
    )
    late_mid, send = call(
        lambda *refs: forward_second(h, *refs), (whole, sent),
        got, other, gain_2, w, copied=(2, 3), scratch=held + (gain_shape, sent[:3]),
    )
    got = exchange(send)
    pieces_1 = swapped_parts(core, (normed, *saved_first), mid_grad, n_fs, d, h)
    near = near_level(core[0], index // 2, *pieces_1)
    send, _ = call(
        update_rows, (sent, (2 * rows, d)), got, own[:rows], early_own, own[rows:], gain_1,
        copied=(4,), scratch=(gain_shape, sent[:3]),
    )
    got = exchange(send)
    pieces = far_level(core[0], index // 8, *near)
    late_out = got[:, :rows].reshape(whole)
    input_grad = got[:, rows:].reshape(whole)
    sums = call(
        lambda *refs: add_gradients(h, *refs), (gate_first.shape + (f32,),) * 6, *pieces, g2,
        sum_gate_first, sum_up_first, sum_down_first.T,
        sum_gate_second, sum_up_second, sum_down_second.T,
        copied=(3,), scratch=(g2.shape,),
    )
    return (
        late_mid, late_out, input_grad,
        sums[0], sums[1], sums[2].T, sums[3], sums[4], sums[5].T,
    )


def solution(mesh):
    rows, w_in, w_out = P("fs", None), P("fs", "tp"), P("tp", "fs")
    weights = (w_in, w_in, w_out) * 2

    return jax.shard_map(
        per_device,
        mesh=mesh,
        in_specs=(rows,) * 4 + (P(), P()) + weights + weights,
        out_specs=(rows,) * 3 + weights,
        check_vma=False,
    )
```

```python
import jax
import jax.numpy as jnp
from jax import lax
from jax.experimental import pallas as pl
from jax.experimental.pallas import tpu as pltpu
from jax.sharding import PartitionSpec as P

norm_eps = 1e-06
f32, bf16 = jnp.float32, jnp.bfloat16


def dot_nn(a, b):
    return jnp.dot(a, b, preferred_element_type=f32)


def dot_nt(a, b):
    return lax.dot_general(a, b, (((1,), (1,)), ((), ())), preferred_element_type=f32)


def dot_tn(a, b):
    return lax.dot_general(a, b, (((0,), (0,)), ((), ())), preferred_element_type=f32)


def row_factor(widened):
    return lax.rsqrt(jnp.mean(widened * widened, axis=-1, keepdims=True) + norm_eps)


def normalize(values, gain):
    widened = values.astype(f32)
    return (widened * row_factor(widened) * gain).astype(bf16)


def widen_cols(a, width):
    return jnp.concatenate([a, jnp.zeros((a.shape[0], width - a.shape[1]), a.dtype)], axis=1)


def forward_part(normed, w_in, w_down, h):
    pre = dot_nn(normed, w_in)
    gate, up = pre[:, :h], pre[:, h : 2 * h]
    hidden = (gate * jax.nn.sigmoid(gate) * up).astype(bf16)
    return dot_nt(widen_cols(hidden, w_down.shape[1]), w_down)


def backward_part(pre, cot, w_in, w_down, h):
    gate, up = pre[:, :h], pre[:, h : 2 * h]
    s = jax.nn.sigmoid(gate)
    activated = gate * s
    hidden = (activated * up).astype(bf16)
    hidden_grad = 0.5 * dot_nn(cot, w_down)[:, :h]
    gate_grad = hidden_grad * up * s * (1.0 + gate * (1.0 - s))
    both = jnp.concatenate([gate_grad, hidden_grad * activated], axis=1).astype(bf16)
    return dot_nt(widen_cols(both, w_in.shape[1]), w_in), both, hidden


def put_rows(send, part, at):
    rows = part.shape[0] // send.shape[0]
    for t in range(send.shape[0]):
        send[t, at : at + rows, :] = part[t * rows : (t + 1) * rows].astype(bf16)


def get_rows(whole, got, at):
    rows = whole.shape[0] // got.shape[0]
    for t in range(got.shape[0]):
        whole[t * rows : (t + 1) * rows, :] = got[t, at : at + rows, :]


def padded(n):
    return -(-n // 128) * 128


def sum_rows(got, at, rows):
    total = got[0, at : at + rows, :].astype(f32)
    for t in range(1, got.shape[0]):
        total = total + got[t, at : at + rows, :].astype(f32)
    return total


def forward_rows(late, branch):
    return (late.astype(f32) + 0.5 * branch).astype(bf16)


def backward_rows(early, cot, gain, normed_grad):
    widened = early.astype(f32)
    factor = row_factor(widened)
    scaled = normed_grad * gain
    unit = widened * factor
    mean = jnp.mean(scaled * unit, axis=-1, keepdims=True)
    return (cot.astype(f32) + factor * (scaled - unit * mean)).astype(bf16)


def start_copies(pairs, sems, first=0):
    copies = [pltpu.make_async_copy(a, b, sems.at[first + k]) for k, (a, b) in enumerate(pairs)]
    for copy in copies:
        copy.start()
    return copies


def weights_of(w, h, block):
    split = padded(2 * h)
    start = block * (split + padded(h))
    return w.at[:, start : start + split], w.at[:, start + split : start + split + padded(h)]


def prepare(at, late, early, mid, cot, gain_1, gain_2, *refs):
    normed, own, held, sems = refs[:3], refs[3:7], refs[7:12], refs[12]
    rows = own[0].shape[0]
    mine = pl.ds(pl.multiple_of(at[0] * rows, rows), rows)
    copies = start_copies(
        (*zip((late, early, mid, gain_1, gain_2), held),
         *((a.at[mine], out) for a, out in zip((late, early, mid, cot), own))),
        sems,
    )
    for copy in copies:
        copy.wait()
    for values, gain, out in zip(held[:3], (held[3], held[3], held[4]), normed):
        out[...] = normalize(values[...], gain[...])


def stage_one(
    h, late, early, cot, w, send, both, hidden,
    v_in, v_down, v_in_1, v_down_1, v_cot, v_b, v_f, sems,
):
    w_in, w_down = weights_of(w, h, 1)
    w_in_1, w_down_1 = weights_of(w, h, 0)
    copies = start_copies(
        (
            (w_in, v_in), (cot, v_cot), (w_down, v_down),
            (w_in_1, v_in_1), (w_down_1, v_down_1),
        ),
        sems,
    )
    copies[0].wait()
    pre = dot_nn(early[...], v_in[...])
    copies[1].wait()
    copies[2].wait()
    part, both[...], hidden[...] = backward_part(pre, v_cot[...], v_in[...], v_down[...], h)
    rows = v_b.shape[1]
    put_rows(v_b, part, 0)
    outs = start_copies(((v_b, send.at[:, rows:, :]),), sems, 5)
    for copy in copies[3:]:
        copy.wait()
    put_rows(v_f, forward_part(late[...], v_in_1[...], v_down_1[...], h), 0)
    outs += start_copies(((v_f, send.at[:, :rows, :]),), sems, 6)
    for copy in outs:
        copy.wait()


def recompute(h, normed, w, pre, v_in, sems):
    (copy,) = start_copies(((weights_of(w, h, 0)[0], v_in),), sems)
    copy.wait()
    pre[...] = dot_nn(normed[...], v_in[...])


def backward_first(h, got, pre, w, cot, other, both, hidden, v_in, v_down, sems):
    w_in, w_down = weights_of(w, h, 0)
    copies = start_copies(((w_down, v_down), (w_in, v_in)), sems)
    get_rows(cot, got, got.shape[1] // 2)
    for copy in copies:
        copy.wait()
    part, both[...], hidden[...] = backward_part(pre[...], cot[...], v_in[...], v_down[...], h)
    put_rows(other, part, 0)


def forward_second(h, got, other, gain, w, late, send, v_in, v_down, v_send, sems):
    w_in, w_down = weights_of(w, h, 1)
    rows = other.shape[1]
    copies = start_copies(((w_in, v_in), (w_down, v_down)), sems)
    get_rows(late, got, 0)
    normed = normalize(late[...], gain[...])
    for t in range(v_send.shape[0]):
        v_send[t, rows:, :] = other[t]
    for copy in copies:
        copy.wait()
    put_rows(v_send, forward_part(normed, v_in[...], v_down[...], h), 0)
    (copy,) = start_copies(((v_send, send),), sems, 2)
    copy.wait()


def update_rows(got, late, early, cot, gain, send, own, v_send, sems):
    rows = late.shape[0]
    own[:rows, :] = forward_rows(late[...], sum_rows(got, 0, rows))
    own[rows:, :] = backward_rows(early[...], cot[...], gain[...], sum_rows(got, rows, rows))
    for t in range(v_send.shape[0]):
        v_send[t] = own[...]
    (copy,) = start_copies(((v_send, send),), sems)
    copy.wait()


def pair_sum(mine, got, out):
    for z in range(out.shape[0]):
        out[z] = (mine[z].astype(f32) + got[z].astype(f32)).astype(bf16)


def near_parts(place, mine, got, *outs):
    for k in range(outs[0].shape[0]):
        for step, out in enumerate(outs):
            at = 4 * k + place[step]
            out[k] = (mine[at].astype(f32) + got[at].astype(f32)).astype(bf16)


def far_parts(place, own, one, back, two, *refs):
    outs, scratch = refs[:-1], refs[-1]
    for k in range(own.shape[0]):
        scratch[k] = (
            own[k].astype(f32) + one[k].astype(f32) + back[k].astype(f32) + two[k].astype(f32)
        ).astype(bf16)
    for step, out in enumerate(outs):
        out[...] = scratch[place[step]]


def add_gradients(h, here, near, far, second, *refs):
    sums, outs, v_second, sems = refs[:6], refs[6:12], refs[12], refs[13]
    (copy,) = start_copies(((second, v_second),), sems)
    copy.wait()
    first = here[...].astype(f32) + near[...].astype(f32) + far[...].astype(f32)
    for block, grads in enumerate((first, v_second[...].astype(f32))):
        for k in range(3):
            outs[3 * block + k][...] = sums[3 * block + k][...] + grads[:, k * h : (k + 1) * h]


def pack_weights(*refs):
    out, held, sems = refs[6], refs[7:13], refs[13]
    rows, h = refs[0].shape
    for copy in start_copies(tuple(zip(refs[:6], held)), sems):
        copy.wait()
    pad_in, pad_down = padded(2 * h) - 2 * h, padded(h) - h
    parts = []
    for gate, up, down in (held[:3], held[3:]):
        zeros = jnp.zeros((rows, pad_in + pad_down), bf16)
        parts += [gate[...], up[...], zeros[:, :pad_in], down[...], zeros[:, :pad_down]]
    out[...] = jnp.concatenate(parts, axis=1)


def block_products(normed, both, hidden, cot, z, size):
    cols = slice(z * size, (z + 1) * size)
    return dot_tn(normed[:, cols], both[...]), 0.5 * dot_tn(cot[:, cols], hidden[...])


def weight_parts_by_core(core, normed, both, hidden, cot, mine, theirs):
    rows, wide = mine.shape[1], both.shape[1]
    first = core[0] == 0
    for z in range(mine.shape[0]):
        for part, cols in zip(
            block_products(normed, both, hidden, cot, z, 2 * rows),
            (slice(0, wide), slice(wide, mine.shape[2])),
        ):
            top, bottom = part[:rows], part[rows:]
            mine[z, :, cols] = jnp.where(first, top, bottom).astype(bf16)
            theirs[z, :, cols] = jnp.where(first, bottom, top).astype(bf16)


def call(body, outs, *args, scalars=0, scratch=(), copied=(), copies=None):
    def typed(shape):
        return (shape[:-1], f32) if shape[-1] is f32 else (shape, bf16)

    def result(shape):
        if shape[-1] is pltpu.HBM:
            return pltpu.HBM(shape[:-1], bf16)
        return jax.ShapeDtypeStruct(*typed(shape))

    spaces = [
        pltpu.SMEM if k < scalars else pltpu.HBM if k in copied else pltpu.VMEM
        for k in range(len(args))
    ]
    sems = [pltpu.SemaphoreType.DMA((copies or len(scratch),))] if copied or copies else []
    return pl.pallas_call(
        body,
        in_specs=[pl.BlockSpec(memory_space=space) for space in spaces],
        out_specs=[
            pl.BlockSpec(memory_space=pltpu.HBM if shape[-1] is pltpu.HBM else pltpu.VMEM)
            for shape in outs
        ],
        out_shape=[result(shape) for shape in outs],
        scratch_shapes=[pltpu.VMEM(*typed(shape)) for shape in scratch] + sems,
        compiler_params=pltpu.CompilerParams(vmem_limit_bytes=48 * 2**20),
    )(*(
        pltpu.with_memory_space_constraint(a, pltpu.HBM) if k in copied else a
        for k, a in enumerate(args)
    ))


def exchange(a):
    return lax.all_to_all(a, "tp", split_axis=0, concat_axis=0, tiled=True)


def moved(a, step, mirror=False):
    n = lax.axis_size("fs")
    sign = [1, -1 if mirror else 1]
    return lax.ppermute(a, "fs", [(q, (q + 2 * step * sign[q % 2]) % n) for q in range(n)])


def swapped(a):
    n = lax.axis_size("fs")
    return lax.ppermute(a, "fs", [(q, q ^ 1) for q in range(n)])


def swapped_parts(core, saved, cot, n_fs, d, h):
    block = (n_fs // 2, d // n_fs, 3 * h)
    mine, theirs = call(weight_parts_by_core, (block, block), core, *saved, cot, scalars=1)
    return mine, swapped(theirs)


def reduce_offloaded(mine, got):
    n = lax.axis_size("fs")
    groups = [[2 * z + c for z in range(n // 2)] for c in range(2)]
    (pair,) = call(pair_sum, (mine.shape,), mine, got)
    return lax.psum_scatter(
        pair.reshape(-1, pair.shape[2]), "fs",
        scatter_dimension=0, tiled=True, axis_index_groups=groups,
    )


def near_level(core, z, mine, got):
    steps = (0, 1, -1, -2)
    classes = jnp.stack([(z + step * (1 - 2 * core)) % 4 for step in steps]).astype(jnp.int32)
    own, *parts = call(
        near_parts, ((4,) + mine.shape[1:],) * 4, classes, mine, got, scalars=1
    )
    return own, *(moved(part, step, mirror=True) for part, step in zip(parts, steps[1:]))


def far_level(core, kz, *parts):
    block = parts[0].shape
    sign = 1 - 2 * core
    place = jnp.stack([(kz + step) % 4 for step in (0, sign, 2, -sign)]).astype(jnp.int32)
    here, on, across, back = call(
        far_parts, (block[1:],) * 4, place, *parts, scalars=1, scratch=(block,)
    )
    across = moved(across, 4, mirror=True)
    back = moved(back, -4, mirror=True)
    on = (on.astype(f32) + across.astype(f32)).astype(bf16)
    return here, moved(on, 4, mirror=True), back


def per_device(
    late_input,
    early_input,
    early_mid,
    cotangent,
    gain_first,
    gain_second,
    gate_first,
    up_first,
    down_first,
    gate_second,
    up_second,
    down_second,
    sum_gate_first,
    sum_up_first,
    sum_down_first,
    sum_gate_second,
    sum_up_second,
    sum_down_second,
):
    h = gate_first.shape[1]
    tokens, d = late_input.shape
    n = lax.axis_size("tp")
    n_fs = lax.axis_size("fs")
    rows = tokens // n
    gain_1, gain_2 = gain_first[None], gain_second[None]
    index = lax.axis_index("fs").astype(jnp.int32)
    core = (index % 2).astype(jnp.int32)[None]
    wide = 2 * (padded(2 * h) + padded(h))
    (packed,) = call(
        pack_weights, ((gate_first.shape[0], wide),),
        gate_first, up_first, down_first.T, gate_second, up_second, down_second.T,
        copied=tuple(range(6)), scratch=(gate_first.shape,) * 6,
    )
    w = lax.all_gather(packed, "fs", axis=0, tiled=True)

    single, whole = (n, rows, d), (tokens, d)
    sent = (n, 2 * rows, d, pltpu.HBM)
    saved_shapes = (whole, (tokens, 2 * h), (tokens, h))
    held = ((d, padded(2 * h)), (d, padded(h)))
    gain_shape = (1, d, f32)
    normed_late, normed, normed_mid, late_own, early_own, mid_own, cot_own = call(
        prepare, (whole,) * 3 + ((rows, d),) * 4, lax.axis_index("tp").astype(jnp.int32)[None],
        late_input, early_input, early_mid, cotangent, gain_1, gain_2,
        scalars=1, copied=tuple(range(1, 7)), scratch=(whole,) * 3 + (gain_shape,) * 2, copies=9,
    )
    send, *saved_second = call(
        lambda *refs: stage_one(h, *refs), (sent,) + saved_shapes[1:],
        normed_late, normed_mid, cotangent, w,
        copied=(2, 3), scratch=held + held + (whole,) + (single,) * 2,
    )
    saved_second = (normed_mid, *saved_second)
    got = exchange(send)
    pieces_2 = swapped_parts(core, saved_second, cotangent, n_fs, d, h)
    (pre,) = call(
        lambda *refs: recompute(h, *refs), ((tokens, padded(2 * h), f32),),
        normed, w, copied=(1,), scratch=held[:1],
    )
    send, own = call(
        update_rows, (sent, (2 * rows, d)), got, late_own, mid_own, cot_own, gain_2,
        scratch=(sent[:3],), copies=1,
    )
    got = exchange(send)
    g2 = reduce_offloaded(*pieces_2)

    mid_grad, other, *saved_first = call(
        lambda *refs: backward_first(h, *refs), (whole, single) + saved_shapes[1:],
        got, pre, w, copied=(2,), scratch=held,
    )
    late_mid, send = call(
        lambda *refs: forward_second(h, *refs), (whole, sent),
        got, other, gain_2, w, copied=(3,), scratch=held + (sent[:3],),
    )
    got = exchange(send)
    pieces_1 = swapped_parts(core, (normed, *saved_first), mid_grad, n_fs, d, h)
    near = near_level(core[0], index // 2, *pieces_1)
    send, _ = call(
        update_rows, (sent, (2 * rows, d)), got, own[:rows], early_own, own[rows:], gain_1,
        scratch=(sent[:3],), copies=1,
    )
    got = exchange(send)
    pieces = far_level(core[0], index // 8, *near)
    late_out = got[:, :rows].reshape(whole)
    input_grad = got[:, rows:].reshape(whole)
    sums = call(
        lambda *refs: add_gradients(h, *refs), (gate_first.shape + (f32,),) * 6, *pieces, g2,
        sum_gate_first, sum_up_first, sum_down_first.T,
        sum_gate_second, sum_up_second, sum_down_second.T,
        copied=(3,), scratch=(g2.shape,),
    )
    return (
        late_mid, late_out, input_grad,
        sums[0], sums[1], sums[2].T, sums[3], sums[4], sums[5].T,
    )


def solution(mesh):
    rows, w_in, w_out = P("fs", None), P("fs", "tp"), P("tp", "fs")
    weights = (w_in, w_in, w_out) * 2

    return jax.shard_map(
        per_device,
        mesh=mesh,
        in_specs=(rows,) * 4 + (P(), P()) + weights + weights,
        out_specs=(rows,) * 3 + weights,
        check_vma=False,
    )
```
